32 devices in a mesh: ep: 16 (over z, y, x), tp: 2 (over core).
Axes of the slice: x: 2, y: 2, z: 4, core: 2. Of those that a mesh axis runs over, the one named last changes fastest.
Arguments:
- stream: bfloat16 [1024, 2048], P('ep', 'tp'), may hold values from -40 to 40
- conv_state: bfloat16 [1024, 3, 2048], P('ep', None, 'tp'), may hold values from -5 to 5
- recur_state: float32 [1024, 2048], P('ep', 'tp'), may hold values from -5 to 5
- mix_gain: float32 [2048], replicated, may hold values from 0.1 to 1.9
- branch_weight: bfloat16 [2048, 2048], P(None, 'tp'), may hold values from -0.125 to 0.125
- gate_weight: bfloat16 [2048, 2048], P(None, 'tp'), may hold values from -0.125 to 0.125
- conv_taps: float32 [4, 2048], P(None, 'tp'), may hold values from -3 to 3
- recur_map: bfloat16 [16, 128, 128], P('tp'), may hold values from -0.5 to 0.5
- input_map: bfloat16 [16, 128, 128], P('tp'), may hold values from -0.5 to 0.5
- decay_logit: float32 [2048], P('tp'), may hold values from -1 to 6
- out_weight: bfloat16 [2048, 2048], P(None, 'tp'), may hold values from -0.125 to 0.125
- moe_gain: float32 [2048], replicated, may hold values from 0.1 to 1.9
- route_ids: int32 [1024, 6], P('ep'), may hold values from 0 to 15, all different within a row; in each aligned block of 64 rows (0 to 63, 64 to 127, ...) at most 64 rows name the same one
- route_weights: float32 [1024, 6], P('ep'), may hold values from 0.2 to 1
- expert_gate: bfloat16 [16, 2048, 512], P('ep', None, 'tp'), may hold values from -0.125 to 0.125
- expert_up: bfloat16 [16, 2048, 512], P('ep', None, 'tp'), may hold values from -0.125 to 0.125
- expert_down: bfloat16 [16, 512, 2048], P('ep', None, 'tp'), may hold values from -0.25 to 0.25
- dense_gate: bfloat16 [2048, 512], P(None, 'tp'), may hold values from -0.125 to 0.125
- dense_up: bfloat16 [2048, 512], P(None, 'tp'), may hold values from -0.125 to 0.125
- dense_down: bfloat16 [512, 2048], P(None, 'tp'), may hold values from -0.25 to 0.25
- dense_scale: float32 [2048], P('tp'), may hold values from 0.1 to 1.9
Outputs:
- result: bfloat16 [1024, 2048], P('ep', 'tp')
- new_state: float32 [1024, 2048], P('ep', 'tp')
- new_conv: bfloat16 [1024, 3, 2048], P('ep', None, 'tp')
The draws below stay inside these ranges and needn't reach their ends.
Inputs may be any that keep to these rules, and one draw needn't show every extreme that they name: `route_ids`: each row names 6 different experts; among the rows of one index of ep no expert is named by more than 64 rows, and in every draw some expert is named by exactly 64 rows of some index.
All inputs are finite; a program needn't handle non-finite values.
Results may differ from the reference program's by a relative error of at most 0.014.
Values may be sent and summed in bfloat16 or wider, within the bound.
A program may use at most 128 MiB of HBM per device.

```python
import math
import jax
import jax.numpy as jnp
import numpy as np
from jax import lax

D = 2048
W = 2048
LBLK = 16
BLK = 128
FFE = 512
FFS = 512
TOP = 6
SEQ_DEV = 64
BATCH = 1024
EXPERTS = 16
CAP = 64
N_EP = 16


def draw_stream(key, part):
    key_cols, key_rows, key_base = jax.random.split(key, 3)
    positions = jnp.arange(D, dtype=jnp.float32) / D
    rough = jnp.exp(jax.random.uniform(key_cols, (D,), jnp.float32, -0.7, 0.7))
    row_scale = jnp.exp(jax.random.uniform(key_rows, (BATCH, 1), jnp.float32, jnp.log(0.5), jnp.log(2.5)))
    column_scale = jnp.exp(jnp.log(3.0) * (positions - 0.5)) * rough
    base = jnp.clip(jax.random.normal(key_base, (BATCH, D), jnp.float32), -4.0, 4.0)
    return (base * column_scale[None, :] * row_scale).astype(jnp.bfloat16)


def levels(rng, shape, cuts, least, high):
    def one(dim, shards_of):
        heights = jax.random.uniform(jax.random.fold_in(jax.random.fold_in(rng, 6), dim), (shards_of,), jnp.float32, least / len(cuts), high / len(cuts))
        return jnp.repeat(jnp.exp(heights), shape[dim] // shards_of).reshape((-1,) + (1,) * (len(shape) - dim - 1))

    level = one(*cuts[0])
    for cut in cuts[1:]:
        level = level * one(*cut)
    return level


def routed_block(key, own, number, rows, count, top, bound, skew):
    order = jax.random.permutation(key, count)
    heavy_load, common = portions_of(count, rows * top, bound, skew, True), portions_of(count, rows * top, bound, skew, False)
    places = jnp.arange(count)

    def named(lengths, offset_by):
        used = int((lengths > 0).sum())
        fixed = max(1, used // 4)
        moved = fixed + (places - fixed + offset_by * (used - fixed)) % max(1, count - fixed)
        return jnp.zeros((count,), jnp.int32).at[order[jnp.where(places < fixed, places, moved)]].set(jnp.asarray(lengths, jnp.int32))

    lengths = jnp.where(number % 4 == 0, named(heavy_load, number // 4), named(common, number - number // 4 - 1))
    mixed = jax.random.permutation(jax.random.fold_in(own, 3), count)
    source_of, taker = mixed[0:count // 2 * 2:2], mixed[1:count // 2 * 2:2]
    slack = jnp.minimum(lengths[source_of] - 1, bound - lengths[taker]) // 2
    slack = jnp.where((source_of == order[0]) | (taker == order[0]) | (lengths[taker] == 0), 0, jnp.maximum(slack, 0))
    moved = jax.random.randint(jax.random.fold_in(own, 4), (count // 2,), 0, 1 << 20) % (slack + 1)
    lengths = lengths.at[source_of].add(-moved).at[taker].add(moved)
    labels = jnp.searchsorted(jnp.cumsum(lengths), jnp.arange(rows * top), side="right").astype(jnp.int32)
    listing = labels.reshape(top, rows).T
    listing = listing[jax.random.permutation(jax.random.fold_in(own, 1), rows)]
    offset_by = jax.random.randint(jax.random.fold_in(own, 2), (rows, 1), 0, top)
    return jnp.take_along_axis(listing, (jnp.arange(top)[None, :] + offset_by) % top, axis=1)


def portions_of(amount, total, limit, lean, full):
    portions = [(1 << 20) // math.isqrt(grade ** lean) + 1 for grade in range(1, amount + 1)]
    largest = limit if full else min(limit, max(-(-total // amount), total * portions[0] // sum(portions)))
    least = 1 if total - largest >= amount - 1 else 0
    counts, surplus = [largest] + [least] * (amount - 1), total - largest - least * (amount - 1)
    while surplus > 0:
        free = [i for i in range(1, amount) if counts[i] < largest] or [i for i in range(1, amount) if counts[i] < limit]
        mass, remaining = sum([portions[i] for i in free]), surplus
        for i in free:
            addition = min(limit - counts[i], max(1, remaining * portions[i] // mass), surplus)
            counts[i] = counts[i] + addition
            surplus = surplus - addition
    return np.array(counts)


def noise(stream_key, shape, spread, limit, cuts=(), kind=jnp.bfloat16):
    array = spread * jax.random.normal(stream_key, shape, jnp.float32)
    if cuts:
        array = array * levels(stream_key, shape, cuts, -0.22, 0.18)
    return jnp.clip(array, -limit, limit).astype(kind)


def setup_inputs(seed: int = 0) -> dict:
    arg_keys = jax.random.split(jax.random.key(seed), 22)
    stream = draw_stream(jax.random.fold_in(arg_keys[21], 71), 0)
    conv_state = noise(arg_keys[1], (BATCH, 3, W), 1.0, 5.0, ((0, 16), (2, 2)))
    recur_state = noise(arg_keys[2], (BATCH, W), 1.0, 5.0, ((0, 16), (1, 2)), jnp.float32)
    mix_gain = jnp.clip(1.0 + 0.18 * jax.random.normal(arg_keys[3], (D,), jnp.float32), 0.1, 1.9)
    branch_weight = noise(arg_keys[4], (D, W), D ** -0.5, 0.125, ((1, 2),))
    gate_weight = noise(arg_keys[5], (D, W), D ** -0.5, 0.125, ((1, 2),))
    conv_taps = noise(arg_keys[6], (4, W), 0.5, 3.0, ((1, 2),), jnp.float32)
    recur_map = noise(arg_keys[7], (LBLK, BLK, BLK), BLK ** -0.5, 0.5, ((0, 2),))
    input_map = noise(arg_keys[8], (LBLK, BLK, BLK), BLK ** -0.5, 0.5, ((0, 2),))
    decay_logit = jnp.clip(-1.0 + 7.0 * jax.random.uniform(arg_keys[9], (W,), jnp.float32) ** levels(arg_keys[9], (W,), ((0, 2),), -0.2, 0.2), -1.0, 6.0)
    out_weight = noise(arg_keys[10], (W, D), W ** -0.5, 0.125, ((1, 2),))
    moe_gain = jnp.clip(1.0 + 0.18 * jax.random.normal(arg_keys[11], (D,), jnp.float32), 0.1, 1.9)
    route_ids_keys = jax.random.split(jax.random.fold_in(arg_keys[12], 1), BATCH // SEQ_DEV)
    route_ids_turns = jax.random.permutation(jax.random.fold_in(arg_keys[12], 3), BATCH // SEQ_DEV)
    route_ids = jax.vmap(lambda own, number: routed_block(jax.random.fold_in(arg_keys[12], 2), own, number, SEQ_DEV, EXPERTS, TOP, CAP, 1))(route_ids_keys, route_ids_turns).reshape((BATCH, TOP))
    route_weights = jnp.clip(0.2 + 0.8 * jax.random.uniform(arg_keys[13], (BATCH, TOP), jnp.float32) ** levels(arg_keys[13], (BATCH, TOP), ((0, 16),), -0.2, 0.2), 0.2, 1.0)
    expert_gate = noise(arg_keys[14], (EXPERTS, D, FFE), D ** -0.5, 0.125, ((0, 16), (2, 2)))
    expert_up = noise(arg_keys[15], (EXPERTS, D, FFE), D ** -0.5, 0.125, ((0, 16), (2, 2)))
    expert_down = noise(arg_keys[16], (EXPERTS, FFE, D), FFE ** -0.5, 0.25, ((0, 16), (2, 2)))
    dense_gate = noise(arg_keys[17], (D, FFS), D ** -0.5, 0.125, ((1, 2),))
    dense_up = noise(arg_keys[18], (D, FFS), D ** -0.5, 0.125, ((1, 2),))
    dense_down = noise(arg_keys[19], (FFS, D), FFS ** -0.5, 0.25, ((1, 2),))
    dense_scale = jnp.clip(1.0 + 0.18 * jax.random.normal(arg_keys[20], (D,), jnp.float32), 0.1, 1.9)
    return dict(stream=stream, conv_state=conv_state, recur_state=recur_state, mix_gain=mix_gain, branch_weight=branch_weight, gate_weight=gate_weight, conv_taps=conv_taps, recur_map=recur_map, input_map=input_map, decay_logit=decay_logit, out_weight=out_weight, moe_gain=moe_gain, route_ids=route_ids, route_weights=route_weights, expert_gate=expert_gate, expert_up=expert_up, expert_down=expert_down, dense_gate=dense_gate, dense_up=dense_up, dense_down=dense_down, dense_scale=dense_scale)


def layer_normed(values, gain_vec):
    widened = values.astype(jnp.float32)
    row_mean = lax.optimization_barrier(jnp.mean(widened, axis=-1, keepdims=True))
    row_var = lax.optimization_barrier(jnp.mean(widened * widened, axis=-1, keepdims=True)) - row_mean * row_mean
    return ((widened - row_mean) * lax.rsqrt(row_var + 1e-05) * gain_vec).astype(jnp.bfloat16)

def gated_rows(inputs, w_gate, w_up, w_down):
    gate_sum = jnp.dot(inputs, w_gate, preferred_element_type=jnp.float32)
    up_sum = jnp.dot(inputs, w_up, preferred_element_type=jnp.float32)
    hidden = (jax.nn.silu(gate_sum) * up_sum).astype(jnp.bfloat16)
    return jnp.dot(hidden, w_down, preferred_element_type=jnp.float32).astype(jnp.bfloat16)

def reference(stream, conv_state, recur_state, mix_gain, branch_weight, gate_weight, conv_taps, recur_map, input_map, decay_logit, out_weight, moe_gain, route_ids, route_weights, expert_gate, expert_up, expert_down, dense_gate, dense_up, dense_down, dense_scale):
    normed = layer_normed(stream, mix_gain)
    branch_in = jnp.dot(normed, branch_weight, preferred_element_type=jnp.float32).astype(jnp.bfloat16)
    gate_pre = jnp.dot(normed, gate_weight, preferred_element_type=jnp.float32).astype(jnp.bfloat16)
    conv_sum = branch_in.astype(jnp.float32) * conv_taps[3]
    for offset in range(3):
        conv_sum = conv_sum + conv_state[:, offset].astype(jnp.float32) * conv_taps[offset]
    conv_out = conv_sum.astype(jnp.bfloat16)
    new_conv = jnp.concatenate([conv_state[:, 1:], branch_in[:, None]], axis=1)
    grouped = conv_out.astype(jnp.float32).reshape(BATCH, LBLK, BLK)
    recur_gate = jax.nn.sigmoid(jnp.einsum('nbc,bcd->nbd', grouped, recur_map.astype(jnp.float32))).reshape(BATCH, W)
    input_gate = jax.nn.sigmoid(jnp.einsum('nbc,bcd->nbd', grouped, input_map.astype(jnp.float32))).reshape(BATCH, W)
    log_decay = -8.0 * recur_gate * jax.nn.softplus(-decay_logit)
    driven = jnp.sqrt(-jnp.expm1(2.0 * log_decay)) * (input_gate * conv_out.astype(jnp.float32))
    new_state = jnp.exp(log_decay) * recur_state + driven
    mixer_in = (jax.nn.gelu(gate_pre.astype(jnp.float32)) * new_state).astype(jnp.bfloat16)
    mixer_out = jnp.dot(mixer_in, out_weight, preferred_element_type=jnp.float32).astype(jnp.bfloat16)
    resid = (stream.astype(jnp.float32) + mixer_out.astype(jnp.float32)).astype(jnp.bfloat16)
    normed_two = layer_normed(resid, moe_gain)
    flat_ids = route_ids.reshape(N_EP, SEQ_DEV * TOP)
    one_hot = (flat_ids[:, :, None] == jnp.arange(EXPERTS, dtype=jnp.int32)[None, None, :]).astype(jnp.int32)
    slot_rank = lax.optimization_barrier(jnp.sum(one_hot * (jnp.cumsum(one_hot, axis=1) - 1), axis=2))
    block_ids = jnp.arange(N_EP, dtype=jnp.int32)[:, None]
    column = (block_ids * CAP + slot_rank).reshape(-1).astype(jnp.int32)
    token_ids = (jnp.arange(BATCH * TOP, dtype=jnp.int32) // TOP).astype(jnp.int32)
    row_token = jnp.full((EXPERTS, N_EP * CAP), BATCH, jnp.int32).at[route_ids.reshape(-1), column].set(token_ids)
    padded = jnp.concatenate([normed_two, jnp.zeros((1, D), jnp.bfloat16)], axis=0)

    def one_expert(packed):
        rows_taken, w_gate, w_up, w_down = packed
        return gated_rows(padded[rows_taken], w_gate, w_up, w_down)
    outputs = lax.map(one_expert, (row_token, expert_gate, expert_up, expert_down))
    picked = outputs[route_ids.reshape(-1), column].reshape(BATCH, TOP, D)
    routed = lax.optimization_barrier(jnp.sum(picked.astype(jnp.float32) * route_weights[:, :, None], axis=1))
    dense_out = gated_rows(normed_two, dense_gate, dense_up, dense_down)
    result = (resid.astype(jnp.float32) + routed + dense_scale * dense_out.astype(jnp.float32)).astype(jnp.bfloat16)
    return (result, new_state, new_conv)
```

```python
import functools

import jax
import jax.numpy as jnp
from jax import lax
from jax.experimental import pallas as pl
from jax.experimental.pallas import tpu as pltpu
from jax.sharding import PartitionSpec as P

BF16 = jnp.bfloat16
F32 = jnp.float32
VMEM = pl.BlockSpec(memory_space=pltpu.VMEM)
ANY = pl.BlockSpec(memory_space=pl.ANY)
HBM = pl.BlockSpec(memory_space=pltpu.HBM)


def dot(a, b):
    return jnp.dot(a, b, preferred_element_type=F32)


def remote(src, dst, send_sem, recv_sem, device):
    return pltpu.make_async_remote_copy(
        src_ref=src,
        dst_ref=dst,
        send_sem=send_sem,
        recv_sem=recv_sem,
        device_id=device,
        device_id_type=pl.DeviceIdType.MESH,
    )


def row_sums(rows):
    return (
        jnp.sum(rows, axis=1, keepdims=True),
        jnp.sum(rows * rows, axis=1, keepdims=True),
    )


def neg_expm1(y):
    series = 1.0 + y / 8.0
    for order in range(7, 1, -1):
        series = 1.0 + y / order * series
    return jnp.where(y > -0.3, -y * series, 1.0 - jnp.exp(y))


def norm_pair(own, own_sums, peer, gain_ref, t, out_ref):
    width = own.shape[1]
    peer_sums = row_sums(peer)
    mean = (own_sums[0] + peer_sums[0]) / (2 * width)
    var = (own_sums[1] + peer_sums[1]) / (2 * width) - mean * mean
    scale = lax.rsqrt(var + 1e-05)
    for slot, (rows, half) in enumerate(((own, t), (peer, 1 - t))):
        out_ref[slot] = ((rows - mean) * scale * gain_ref[half]).astype(BF16)


def mixer_kernel(
    stream_ref,
    part_ref,
    state_ref,
    gain_ref,
    branch_hbm,
    gate_hbm,
    taps_ref,
    rmap_ref,
    imap_ref,
    decay_ref,
    out_hbm,
    gain2_ref,
    branch_ref,
    new_state_ref,
    resid_ref,
    n2_ref,
    branch_w,
    gate_w,
    out_w,
    peer_ref,
    nrm_ref,
    mix_ref,
    res_ref,
    load_sem,
    send_sem,
    recv_sem,
):
    t = lax.axis_index("tp")
    partner = {"tp": 1 - t}
    loads = [
        pltpu.make_async_copy(src, dst, load_sem.at[i])
        for i, (src, dst) in enumerate(
            ((branch_hbm, branch_w), (gate_hbm, gate_w), (out_hbm, out_w))
        )
    ]
    for load in loads:
        load.start()
    barrier = pltpu.get_barrier_semaphore()
    pl.semaphore_signal(barrier, inc=1, device_id=partner, device_id_type=pl.DeviceIdType.MESH)
    pl.semaphore_wait(barrier, 1)
    first = remote(stream_ref, peer_ref, send_sem.at[0], recv_sem.at[0], partner)
    first.start()
    own = stream_ref[...].astype(F32)
    own_sums = row_sums(own)
    first.wait_recv()
    norm_pair(own, own_sums, peer_ref[...].astype(F32), gain_ref, t, nrm_ref)

    width = stream_ref.shape[1]
    block = rmap_ref.shape[1]
    chunk = 2 * block
    loads[0].wait()
    loads[1].wait()
    for c in range(width // chunk):
        cols = pl.ds(c * chunk, chunk)
        branch = dot(nrm_ref[0], branch_w[t, :, cols]) + dot(nrm_ref[1], branch_w[1 - t, :, cols])
        branch = branch.astype(BF16)
        branch_ref[:, cols] = branch
        gate = dot(nrm_ref[0], gate_w[t, :, cols]) + dot(nrm_ref[1], gate_w[1 - t, :, cols])
        gate = gate.astype(BF16).astype(F32)
        conv = (branch.astype(F32) * taps_ref[3:4, cols] + part_ref[:, cols]).astype(BF16)
        rec, inp = [], []
        for b in range(2):
            piece = conv[:, b * block : (b + 1) * block]
            rec.append(dot(piece, rmap_ref[2 * c + b]))
            inp.append(dot(piece, imap_ref[2 * c + b]))
        recur_gate = jax.nn.sigmoid(jnp.concatenate(rec, axis=1))
        input_gate = jax.nn.sigmoid(jnp.concatenate(inp, axis=1))
        logit = -decay_ref[:, cols]
        softplus = jnp.maximum(logit, 0.0) + jnp.log1p(jnp.exp(-jnp.abs(logit)))
        log_decay = -8.0 * recur_gate * softplus
        driven = jnp.sqrt(neg_expm1(2.0 * log_decay)) * (input_gate * conv.astype(F32))
        state = jnp.exp(log_decay) * state_ref[:, cols] + driven
        new_state_ref[:, cols] = state
        gelu = 0.5 * gate * (1.0 + jnp.tanh(0.7978845608028654 * (gate + 0.044715 * gate**3)))
        mix_ref[0, :, cols] = (gelu * state).astype(BF16)
    second = remote(mix_ref.at[0], mix_ref.at[1], send_sem.at[1], recv_sem.at[1], partner)
    second.start()
    loads[2].wait()
    mixed = dot(mix_ref[0], out_w[t])
    second.wait_recv()
    mixed = (mixed + dot(mix_ref[1], out_w[1 - t])).astype(BF16)
    resid = (own + mixed.astype(F32)).astype(BF16)
    res_ref[0] = resid
    third = remote(res_ref.at[0], res_ref.at[1], send_sem.at[2], recv_sem.at[2], partner)
    third.start()
    resid_ref[...] = resid
    resid = resid.astype(F32)
    sums = row_sums(resid)
    third.wait_recv()
    norm_pair(resid, sums, res_ref[1].astype(F32), gain2_ref, t, n2_ref)
    for copy in (first, second, third):
        copy.wait_send()


def flipped(q, r):
    return (q // 2 + r // 2) % 2 * 2 + (q + r) % 2


def layer_kernel(
    peers,
    stream_hbm,
    conv_hbm,
    state_hbm,
    gain_hbm,
    branch_hbm,
    gate_hbm,
    taps_hbm,
    rmap_hbm,
    imap_hbm,
    decay_hbm,
    out_hbm,
    gain2_hbm,
    ids_hbm,
    weights_hbm,
    scale_hbm,
    eg_hbm,
    eu_hbm,
    ed_hbm,
    dg_hbm,
    du_hbm,
    dd_hbm,
    result_ref,
    new_state_ref,
    new_conv_ref,
    stream_ref,
    conv_ref,
    state_ref,
    gain_ref,
    branch_w,
    gate_w,
    taps_ref,
    rmap_ref,
    imap_ref,
    decay_ref,
    out_w,
    gain2_ref,
    ids_ref,
    weights_ref,
    scale_ref,
    eg,
    eu,
    ed,
    dg,
    du,
    dd,
    peer_ref,
    nrm_ref,
    mix_ref,
    res_ref,
    inc,
    hid,
    dhid,
    snd,
    zbuf,
    got_d,
    got_x,
    got_y,
    got_z,
    base_ref,
    wsend,
    wrecv,
    load_sem,
    m_send,
    m_recv,
    w_send,
    w_recv,
    p_send,
    p_recv,
    h_send,
    h_recv,
    link_send,
    link_recv,
    back_send,
    back_recv,
):
    e = lax.axis_index("ep")
    t = lax.axis_index("tp")
    partner = {"tp": 1 - t}
    depth = peers // 4
    z = e // 4
    q = e % 4
    x_near = {"ep": 4 * z + flipped(q, 1)}
    y_near = {"ep": 4 * z + flipped(q, 2)}
    rows, width = stream_ref.shape
    pairs = (
        (stream_hbm, stream_ref),
        (gain_hbm, gain_ref),
        (branch_hbm, branch_w),
        (gate_hbm, gate_w),
        (conv_hbm, conv_ref),
        (taps_hbm, taps_ref),
        (rmap_hbm, rmap_ref),
        (imap_hbm, imap_ref),
        (decay_hbm, decay_ref),
        (state_hbm, state_ref),
        (out_hbm, out_w),
        (gain2_hbm, gain2_ref),
        (ids_hbm, ids_ref),
        (weights_hbm, weights_ref),
        (scale_hbm, scale_ref),
        (dg_hbm, dg),
        (du_hbm, du),
        (dd_hbm, dd),
        (eg_hbm, eg),
        (eu_hbm, eu),
        (ed_hbm, ed),
    )
    loads = [pltpu.make_async_copy(a, b, load_sem.at[i]) for i, (a, b) in enumerate(pairs)]
    for i in (0, 1, 12, 13, 2, 3, 4, 5, 6, 7, 8, 9):
        loads[i].start()
    barrier = pltpu.get_barrier_semaphore()
    pl.semaphore_signal(barrier, inc=1, device_id=partner, device_id_type=pl.DeviceIdType.MESH)

    @pl.loop(1, peers)
    def _(offset):
        pl.semaphore_signal(
            barrier,
            inc=1,
            device_id={"ep": lax.rem(e + offset, peers)},
            device_id_type=pl.DeviceIdType.MESH,
        )

    loads[0].wait()
    pl.semaphore_wait(barrier, peers)
    first = remote(stream_ref, peer_ref, m_send.at[0], m_recv.at[0], partner)
    first.start()
    own = stream_ref[...].astype(F32)
    own_sums = row_sums(own)

    loads[12].wait()
    loads[13].wait()
    ids = ids_ref[...]
    weights = weights_ref[...]
    lanes = wsend.shape[2]
    for d in range(peers):
        row = jnp.sum(jnp.where(ids == d, weights, 0.0), axis=0, keepdims=True)
        wsend[d] = jnp.concatenate([row, jnp.zeros((1, lanes - rows), F32)], axis=1)

    def weighing(r, o):
        there = (z + o) % depth
        d = 4 * there + flipped(q, r)
        slot = 4 * z + r
        return remote(wsend.at[d], wrecv.at[slot], w_send.at[d], w_recv.at[slot], {"ep": d})

    places = [(r, o) for r in range(4) for o in range(depth) if r or o]
    for r, o in places:
        weighing(r, o).start()

    loads[1].wait()
    first.wait_recv()
    norm_pair(own, own_sums, peer_ref[...].astype(F32), gain_ref, t, nrm_ref)
    for load in loads[2:10]:
        load.wait()
    for i in (10, 11, 14, 15, 16, 17, 18, 19, 20):
        loads[i].start()
    block = rmap_ref.shape[1]
    chunk = 2 * block
    for c in range(width // chunk):
        cols = pl.ds(c * chunk, chunk)
        branch = dot(nrm_ref[0], branch_w[t, :, cols]) + dot(nrm_ref[1], branch_w[1 - t, :, cols])
        branch = branch.astype(BF16)
        gate = dot(nrm_ref[0], gate_w[t, :, cols]) + dot(nrm_ref[1], gate_w[1 - t, :, cols])
        gate = gate.astype(BF16).astype(F32)
        conv = branch.astype(F32) * taps_ref[3:4, cols]
        for i in range(3):
            conv = conv + conv_ref[i, :, cols].astype(F32) * taps_ref[i : i + 1, cols]
        conv = conv.astype(BF16)
        new_conv_ref[0, :, cols] = conv_ref[1, :, cols]
        new_conv_ref[1, :, cols] = conv_ref[2, :, cols]
        new_conv_ref[2, :, cols] = branch
        rec, inp = [], []
        for b in range(2):
            piece = conv[:, b * block : (b + 1) * block]
            rec.append(dot(piece, rmap_ref[2 * c + b]))
            inp.append(dot(piece, imap_ref[2 * c + b]))
        recur_gate = jax.nn.sigmoid(jnp.concatenate(rec, axis=1))
        input_gate = jax.nn.sigmoid(jnp.concatenate(inp, axis=1))
        logit = -decay_ref[:, cols]
        softplus = jnp.maximum(logit, 0.0) + jnp.log1p(jnp.exp(-jnp.abs(logit)))
        log_decay = -8.0 * recur_gate * softplus
        driven = jnp.sqrt(neg_expm1(2.0 * log_decay)) * (input_gate * conv.astype(F32))
        state = jnp.exp(log_decay) * state_ref[:, cols] + driven
        new_state_ref[:, cols] = state
        gelu = 0.5 * gate * (1.0 + jnp.tanh(0.7978845608028654 * (gate + 0.044715 * gate**3)))
        mix_ref[0, :, cols] = (gelu * state).astype(BF16)
    second = remote(mix_ref.at[0], mix_ref.at[1], m_send.at[1], m_recv.at[1], partner)
    second.start()
    loads[10].wait()
    mixed = dot(mix_ref[0], out_w[t])
    second.wait_recv()
    mixed = (mixed + dot(mix_ref[1], out_w[1 - t])).astype(BF16)
    resid = (own + mixed.astype(F32)).astype(BF16)
    res_ref[0] = resid
    third = remote(res_ref.at[0], res_ref.at[1], m_send.at[2], m_recv.at[2], partner)
    third.start()
    resid = resid.astype(F32)
    sums = row_sums(resid)
    loads[11].wait()
    third.wait_recv()
    norm_pair(resid, sums, res_ref[1].astype(F32), gain2_ref, t, nrm_ref)
    inc[0, 4 * z] = nrm_ref[0]
    inc[1, 4 * z] = nrm_ref[1]

    split = width // 2

    def at(o):
        return (z + depth - o) % depth

    def z_copy(o):
        there = {"ep": 4 * ((z + o) % depth) + q}
        return remote(
            inc.at[0, 4 * z], inc.at[0, 4 * z], link_send.at[0, o], link_recv.at[0, z], there
        )

    def z_wait(o):
        j = at(o)
        mine = inc.at[0, 4 * j]
        remote(mine, mine, link_send.at[0, o], link_recv.at[0, j], partner).wait_recv()

    def side_copy(r, o):
        j = at(o)
        return remote(
            inc.at[0, 4 * j],
            inc.at[0, 4 * j + r],
            link_send.at[r, j],
            link_recv.at[r, j],
            x_near if r == 1 else y_near,
        )

    def d_copy(r, o):
        j = at(o)
        cols = pl.ds((r - 1) * split, split)
        return remote(
            inc.at[0, 4 * j + 3 - r, :, cols],
            inc.at[0, 4 * j + 3, :, cols],
            link_send.at[2 + r, j],
            link_recv.at[2 + r, j],
            x_near if r == 1 else y_near,
        )

    def p_copy(r, o):
        slot = 4 * at(o) + r
        return remote(inc.at[0, slot], inc.at[1, slot], p_send.at[slot], p_recv.at[slot], partner)

    for o in range(1, depth):
        z_copy(o).start()
    side_copy(1, 0).start()
    side_copy(2, 0).start()

    for load in loads[14:18]:
        load.wait()
    dense_gate = dot(nrm_ref[0], dg[t]) + dot(nrm_ref[1], dg[1 - t])
    dense_up = dot(nrm_ref[0], du[t]) + dot(nrm_ref[1], du[1 - t])
    dhid[0] = (jax.nn.silu(dense_gate) * dense_up).astype(BF16)
    dense_copy = remote(dhid.at[0], dhid.at[1], m_send.at[3], m_recv.at[3], partner)
    dense_copy.start()

    def along(o):
        z_wait(o)
        side_copy(1, o).start()
        side_copy(2, o).start()
        p_copy(0, o).start()

    def near(o):
        side_copy(1, o).wait_recv()
        d_copy(2, o).start()
        p_copy(1, o).start()
        side_copy(2, o).wait_recv()
        d_copy(1, o).start()
        p_copy(2, o).start()

    def h_copy(o):
        part = pl.ds(4 * at(o), 4)
        return remote(hid.at[0, part], hid.at[1, part], h_send.at[o], h_recv.at[o], partner)

    def upward(o):
        for r in range(4):
            if r or o:
                p_copy(r, o).wait_recv()
        part = pl.ds(4 * at(o), 4)
        mine = inc[0, part].reshape(4 * rows, width)
        peer = inc[1, part].reshape(4 * rows, width)
        gate = dot(mine, eg[t]) + dot(peer, eg[1 - t])
        up = dot(mine, eu[t]) + dot(peer, eu[1 - t])
        hid[0, part] = (jax.nn.silu(gate) * up).astype(BF16).reshape(4, rows, -1)
        h_copy(o).start()

    spread = lax.broadcasted_iota(jnp.int32, (rows, lanes), 0) == lax.broadcasted_iota(
        jnp.int32, (rows, lanes), 1
    )

    def downward(o):
        base_slot = 4 * at(o)
        part = pl.ds(base_slot, 4)
        cols = []
        for r in range(4):
            row = wrecv[base_slot + r]
            cols.append(jnp.sum(jnp.where(spread, row, 0.0), axis=1, keepdims=True))
        h_copy(o).wait_recv()
        mine = hid[0, part].reshape(4 * rows, -1)
        peer = hid[1, part].reshape(4 * rows, -1)
        served = dot(mine, ed[t]) + dot(peer, ed[1 - t])
        served = served * jnp.concatenate(cols, axis=0)
        snd[part] = served.astype(BF16).reshape(4, rows, width)
        bd_copy(1, o).start()
        bd_copy(2, o).start()

    def bd_copy(r, o):
        j = at(o)
        cols = pl.ds((r - 1) * split, split)
        return remote(
            snd.at[4 * j + 3, :, cols],
            got_d.at[j, :, cols],
            back_send.at[2 + r, j],
            back_recv.at[2 + r, j],
            x_near if r == 1 else y_near,
        )

    def side_back(r, o):
        j = at(o)
        return remote(
            snd.at[4 * j + r],
            (got_x if r == 1 else got_y).at[j],
            back_send.at[r, j],
            back_recv.at[r, j],
            x_near if r == 1 else y_near,
        )

    def bz_copy(o):
        j = at(o)
        there = {"ep": 4 * j + q}
        return remote(zbuf.at[j], got_z.at[z], back_send.at[0, j], back_recv.at[0, z], there)

    def bz_wait(o):
        j = at(o)
        remote(zbuf.at[j], got_z.at[j], back_send.at[0, j], back_recv.at[0, j], partner).wait_recv()

    def joined(o):
        j = at(o)
        for r in (1, 2):
            bd_copy(r, o).wait_recv()
            cols = pl.ds((r - 1) * split, split)
            slot = 4 * j + 3 - r
            both = snd[slot, :, cols].astype(F32) + got_d[j, :, cols].astype(F32)
            snd[slot, :, cols] = both.astype(BF16)
            side_back(3 - r, o).start()

    def summed(o):
        j = at(o)
        side_back(1, o).wait_recv()
        side_back(2, o).wait_recv()
        total = snd[4 * j].astype(F32) + got_x[j].astype(F32) + got_y[j].astype(F32)
        if o:
            zbuf[j] = total.astype(BF16)
            bz_copy(o).start()
        return total

    along(1)
    near(0)
    for r, o in places:
        slot = 4 * at(o) + r
        remote(wsend.at[0], wrecv.at[slot], w_send.at[0], w_recv.at[slot], partner).wait_recv()
    mine = jnp.sum(jnp.where(ids == e, weights, 0.0), axis=0, keepdims=True)
    wrecv[4 * z] = jnp.concatenate([mine, jnp.zeros((1, lanes - rows), F32)], axis=1)
    dense = dot(dhid[0], dd[t])
    dense_copy.wait_recv()
    dense = (dense + dot(dhid[1], dd[1 - t])).astype(BF16)
    base_ref[...] = resid + scale_ref[...] * dense.astype(F32)
    for load in loads[18:]:
        load.wait()

    for step in range(1, depth + 3):
        if step + 1 < depth:
            along(step + 1)
        if step < depth:
            near(step)
        if step <= depth:
            d_copy(1, step - 1).wait_recv()
            d_copy(2, step - 1).wait_recv()
            p_copy(3, step - 1).start()
        if 2 <= step <= depth + 1:
            joined(step - 2)
        if step <= depth:
            upward(step - 1)
            downward(step - 1)
        if 3 <= step:
            part_sum = summed(step - 3)
            if step == 3:
                base_ref[...] += part_sum
    total = base_ref[...]
    for o in range(1, depth):
        bz_wait(o)
        total = total + got_z[at(o)].astype(F32)
    result_ref[...] = total.astype(BF16)

    for copy in (first, second, third, dense_copy):
        copy.wait_send()
    for r, o in places:
        weighing(r, o).wait_send()
        p_copy(r, o).wait_send()
    for o in range(depth):
        h_copy(o).wait_send()
        if o:
            z_copy(o).wait_send()
            bz_copy(o).wait_send()
        for r in (1, 2):
            for copy in (side_copy, d_copy, side_back, bd_copy):
                copy(r, o).wait_send()


def expert_kernel(
    full,
    peers,
    group,
    n2_ref,
    out_ref,
    resid_ref,
    ids_ref,
    weights_ref,
    scale_ref,
    eg_hbm,
    eu_hbm,
    ed_hbm,
    dg_hbm,
    du_hbm,
    dd_hbm,
    *refs,
):
    if full:
        result_ref, *refs = refs
    else:
        dense_ref, back_ref, *refs = refs
    (
        eg,
        eu,
        ed,
        dg,
        du,
        dd,
        inc,
        hid,
        src,
        ret,
        dhid,
        load_sem,
        own_sem,
        x_send,
        x_recv,
        f_send,
        f_recv,
        h_send,
        h_recv,
        r_send,
        r_recv,
        d_sem,
    ) = refs
    e = lax.axis_index("ep")
    t = lax.axis_index("tp")
    partner = {"tp": 1 - t}
    groups = peers // group
    cap = inc.shape[2]
    width = inc.shape[3]
    loads = [
        pltpu.make_async_copy(a, b, load_sem.at[i])
        for i, (a, b) in enumerate(
            ((dg_hbm, dg), (du_hbm, du), (dd_hbm, dd), (eg_hbm, eg), (eu_hbm, eu), (ed_hbm, ed))
        )
    ]
    for load in loads:
        load.start()

    def outgoing(offset):
        return n2_ref.at[0] if full else out_ref.at[lax.rem(e + offset, peers)]

    keep = pltpu.make_async_copy(outgoing(0), inc.at[0, 0], own_sem)
    keep.start()
    barrier = pltpu.get_barrier_semaphore()
    pl.semaphore_signal(barrier, inc=1, device_id=partner, device_id_type=pl.DeviceIdType.MESH)

    @pl.loop(1, peers)
    def _(offset):
        pl.semaphore_signal(
            barrier,
            inc=1,
            device_id={"ep": lax.rem(e + offset, peers)},
            device_id_type=pl.DeviceIdType.MESH,
        )

    pl.semaphore_wait(barrier, peers)

    def sending(offset):
        return remote(
            outgoing(offset),
            inc.at[0, offset],
            x_send.at[offset],
            x_recv.at[offset],
            {"ep": lax.rem(e + offset, peers)},
        )

    @pl.loop(1, peers)
    def _(offset):
        sending(offset).start()

    for load in loads[:3]:
        load.wait()
    rows0, rows1 = n2_ref[0], n2_ref[1]
    dense_gate = dot(rows0, dg[t]) + dot(rows1, dg[1 - t])
    dense_up = dot(rows0, du[t]) + dot(rows1, du[1 - t])
    dhid[0] = (jax.nn.silu(dense_gate) * dense_up).astype(BF16)
    dense_copy = remote(dhid.at[0], dhid.at[1], d_sem.at[0], d_sem.at[1], partner)
    dense_copy.start()
    dense = dot(dhid[0], dd[t])
    dense_copy.wait()
    dense = (dense + dot(dhid[1], dd[1 - t])).astype(BF16)
    keep.wait()
    for load in loads[3:]:
        load.wait()

    def forwarding(g):
        part = pl.ds(g * group, group)
        return remote(inc.at[0, part], inc.at[1, part], f_send.at[g], f_recv.at[g], partner)

    def hiding(g):
        part = pl.ds(g * group, group)
        return remote(hid.at[0, part], hid.at[1, part], h_send.at[g], h_recv.at[g], partner)

    def returning(offset):
        return remote(
            src.at[offset],
            ret.at[offset],
            r_send.at[offset],
            r_recv.at[offset],
            {"ep": lax.rem(e + peers - offset, peers)},
        )

    def arrive(g):
        @pl.loop(max(1, g * group), (g + 1) * group)
        def _(offset):
            sending(offset).wait_recv()

        forwarding(g).start()

    def upward(g):
        forwarding(g).wait_recv()
        part = pl.ds(g * group, group)
        own = inc[0, part].reshape(group * cap, width)
        peer = inc[1, part].reshape(group * cap, width)
        gate = dot(own, eg[t]) + dot(peer, eg[1 - t])
        up = dot(own, eu[t]) + dot(peer, eu[1 - t])
        hidden = (jax.nn.silu(gate) * up).astype(BF16)
        hid[0, part] = hidden.reshape(group, cap, -1)
        hiding(g).start()

    def downward(g):
        hiding(g).wait_recv()
        part = pl.ds(g * group, group)
        own = hid[0, part].reshape(group * cap, -1)
        peer = hid[1, part].reshape(group * cap, -1)
        served = dot(own, ed[t]) + dot(peer, ed[1 - t])
        src[part] = served.astype(BF16).reshape(group, cap, width)

        @pl.loop(max(1, g * group), (g + 1) * group)
        def _(offset):
            returning(offset).start()

    for step in range(groups + 2):
        if step < groups:
            arrive(step)
        if 1 <= step <= groups:
            upward(step - 1)
        if step >= 2:
            downward(step - 2)

    if full:
        total = resid_ref[...].astype(F32) + scale_ref[...] * dense.astype(F32)
        ids = ids_ref[...]
        weights = weights_ref[...]

        def weight(offset):
            chosen = ids == lax.rem(e + offset, peers)
            return jnp.sum(jnp.where(chosen, weights, 0.0), axis=1, keepdims=True)

        routed = weight(0) * src[0].astype(F32)
        for offset in range(1, peers):
            returning(offset).wait_recv()
            routed = routed + weight(offset) * ret[offset].astype(F32)
        result_ref[...] = (total + routed).astype(BF16)
    else:
        dense_ref[...] = dense
        back_ref[0] = src[0]

        @pl.loop(1, peers)
        def _(offset):
            returning(offset).wait_recv()
            back_ref[offset] = ret[offset]

    @pl.loop(1, peers)
    def _(offset):
        sending(offset).wait_send()
        returning(offset).wait_send()

    @pl.loop(0, groups)
    def _(g):
        forwarding(g).wait_send()
        hiding(g).wait_send()


def emit_kernel(a_in, b_in, c_in, a_out, b_out, c_out, a, b, c, sem):
    sets = tuple(enumerate(((a_in, a, a_out), (b_in, b, b_out), (c_in, c, c_out))))
    reads = [pltpu.make_async_copy(src, mid, sem.at[0, i]) for i, (src, mid, _) in sets]
    writes = [pltpu.make_async_copy(mid, dst, sem.at[1, i]) for i, (_, mid, dst) in sets]
    for read in reads:
        read.start()
    for read, write in zip(reads, writes):
        read.wait()
        write.start()
    for write in writes:
        write.wait()


def halves(weight):
    return weight.reshape(2, weight.shape[0] // 2, weight.shape[1])


def per_device(
    stream,
    conv_state,
    recur_state,
    mix_gain,
    branch_weight,
    gate_weight,
    conv_taps,
    recur_map,
    input_map,
    decay_logit,
    out_weight,
    moe_gain,
    route_ids,
    route_weights,
    expert_gate,
    expert_up,
    expert_down,
    dense_gate,
    dense_up,
    dense_down,
    dense_scale,
):
    rows, width = stream.shape
    dma = pltpu.SemaphoreType.DMA
    top = route_ids.shape[1]
    peers = lax.axis_size("ep")
    cap = max(2, min(rows, 3 * rows * top // peers))
    if cap == rows and peers % 8 == 0:
        operands = (
            stream,
            conv_state.transpose(1, 0, 2),
            recur_state,
            mix_gain.reshape(2, 1, width),
            halves(branch_weight),
            halves(gate_weight),
            conv_taps,
            recur_map,
            input_map,
            decay_logit.reshape(1, width),
            halves(out_weight),
            moe_gain.reshape(2, 1, width),
            route_ids.T,
            route_weights.T,
            dense_scale.reshape(1, width),
            halves(expert_gate[0]),
            halves(expert_up[0]),
            halves(expert_down[0]),
            halves(dense_gate),
            halves(dense_up),
            halves(dense_down),
        )
        depth = peers // 4
        hidden = expert_gate.shape[2]
        lanes = -(-rows // 128) * 128
        column = pltpu.VMEM((depth, rows, width), BF16)
        result, new_state, new_conv = pl.pallas_call(
            functools.partial(layer_kernel, peers),
            out_shape=(
                jax.ShapeDtypeStruct((rows, width), BF16),
                jax.ShapeDtypeStruct((rows, width), F32),
                jax.ShapeDtypeStruct((3, rows, width), BF16),
            ),
            in_specs=[HBM] * len(operands),
            out_specs=[VMEM] * 3,
            scratch_shapes=[pltpu.VMEM(a.shape, a.dtype) for a in operands]
            + [pltpu.VMEM((rows, width), BF16)]
            + [pltpu.VMEM((2, rows, width), BF16)] * 3
            + [
                pltpu.VMEM((2, peers, rows, width), BF16),
                pltpu.VMEM((2, peers, rows, hidden), BF16),
                pltpu.VMEM((2, rows, dense_gate.shape[1]), BF16),
                pltpu.VMEM((peers, rows, width), BF16),
            ]
            + [column] * 5
            + [pltpu.VMEM((rows, width), F32)]
            + [pltpu.VMEM((peers, 1, lanes), F32)] * 2
            + [dma((len(operands),))]
            + [dma((4,))] * 2
            + [dma((peers,))] * 4
            + [dma((depth,))] * 2
            + [dma((5, depth))] * 4,
            compiler_params=pltpu.CompilerParams(
                collective_id=2, has_side_effects=True, vmem_limit_bytes=63 * 1024 * 1024
            ),
            name="layer",
        )(*operands)
        result, new_state, new_conv = pl.pallas_call(
            emit_kernel,
            out_shape=tuple(jax.ShapeDtypeStruct(a.shape, a.dtype) for a in (result, new_state, new_conv)),
            in_specs=[ANY] * 3,
            out_specs=[ANY] * 3,
            scratch_shapes=[pltpu.VMEM(a.shape, a.dtype) for a in (result, new_state, new_conv)]
            + [dma((2, 3))],
            compiler_params=pltpu.CompilerParams(vmem_limit_bytes=63 * 1024 * 1024),
            name="emit",
        )(result, new_state, new_conv)
        return result, new_state, new_conv.transpose(1, 0, 2)
    conv_part = sum(conv_state[:, i].astype(F32) * conv_taps[i] for i in range(3))
    branch_in, new_state, resid, n2 = pl.pallas_call(
        mixer_kernel,
        out_shape=(
            jax.ShapeDtypeStruct((rows, width), BF16),
            jax.ShapeDtypeStruct((rows, width), F32),
            jax.ShapeDtypeStruct((rows, width), BF16),
            jax.ShapeDtypeStruct((2, rows, width), BF16),
        ),
        in_specs=[VMEM] * 4 + [ANY] * 2 + [VMEM] * 4 + [ANY, VMEM],
        out_specs=[VMEM] * 4,
        scratch_shapes=[pltpu.VMEM((2, width, width), BF16)] * 3
        + [pltpu.VMEM((rows, width), BF16)]
        + [pltpu.VMEM((2, rows, width), BF16)] * 3
        + [dma((3,))] * 3,
        compiler_params=pltpu.CompilerParams(
            collective_id=0, has_side_effects=True, vmem_limit_bytes=48 * 1024 * 1024
        ),
        name="mixer",
    )(
        stream,
        conv_part,
        recur_state,
        mix_gain.reshape(2, 1, width),
        halves(branch_weight),
        halves(gate_weight),
        conv_taps,
        recur_map,
        input_map,
        decay_logit.reshape(1, width),
        halves(out_weight),
        moe_gain.reshape(2, 1, width),
    )
    new_conv = jnp.concatenate([conv_state[:, 1:], branch_in[:, None]], axis=1)

    full = cap == rows
    if full:
        outgoing = jnp.zeros((8, 128), BF16)
    else:
        cap = -(-cap // 16) * 16
        flat_ids = route_ids.reshape(-1)
        one_hot = (flat_ids[:, None] == jnp.arange(peers, dtype=jnp.int32)[None, :]).astype(jnp.int32)
        rank = jnp.sum(one_hot * (jnp.cumsum(one_hot, axis=0) - 1), axis=1)
        slots = (flat_ids * cap + rank).reshape(rows, top)
        table = jnp.sum(
            (slots[:, :, None] == jnp.arange(peers * cap, dtype=jnp.int32)).astype(BF16), axis=1
        )
        outgoing = lax.dot_general(
            table, n2[0], (((0,), (0,)), ((), ())), preferred_element_type=F32
        )
        outgoing = outgoing.astype(BF16).reshape(peers, cap, width)
    group = max(1, min(peers, 256 // cap))
    while peers % group:
        group -= 1
    groups = peers // group
    hidden = expert_gate.shape[2]
    out_shape = [jax.ShapeDtypeStruct((rows, width), BF16)]
    if not full:
        out_shape.append(jax.ShapeDtypeStruct((peers, cap, width), BF16))
    outs = pl.pallas_call(
        functools.partial(expert_kernel, full, peers, group),
        out_shape=out_shape,
        in_specs=[VMEM] * 6 + [ANY] * 6,
        out_specs=[VMEM] * len(out_shape),
        scratch_shapes=[
            pltpu.VMEM((2, width, hidden), BF16),
            pltpu.VMEM((2, width, hidden), BF16),
            pltpu.VMEM((2, hidden, width), BF16),
            pltpu.VMEM((2, width, dense_gate.shape[1]), BF16),
            pltpu.VMEM((2, width, dense_gate.shape[1]), BF16),
            pltpu.VMEM((2, dense_gate.shape[1], width), BF16),
            pltpu.VMEM((2, peers, cap, width), BF16),
            pltpu.VMEM((2, peers, cap, hidden), BF16),
            pltpu.VMEM((peers, cap, width), BF16),
            pltpu.VMEM((peers, cap, width), BF16),
            pltpu.VMEM((2, rows, dense_gate.shape[1]), BF16),
            dma((6,)),
            dma,
            dma((peers,)),
            dma((peers,)),
            dma((groups,)),
            dma((groups,)),
            dma((groups,)),
            dma((groups,)),
            dma((peers,)),
            dma((peers,)),
            dma((2,)),
        ],
        compiler_params=pltpu.CompilerParams(
            collective_id=1, has_side_effects=True, vmem_limit_bytes=56 * 1024 * 1024
        ),
        name="experts",
    )(
        n2,
        outgoing,
        resid,
        route_ids,
        route_weights,
        dense_scale.reshape(1, width),
        halves(expert_gate[0]),
        halves(expert_up[0]),
        halves(expert_down[0]),
        halves(dense_gate),
        halves(dense_up),
        halves(dense_down),
    )
    if full:
        return outs[0], new_state, new_conv
    dense_out, back = outs
    shifted = lax.rem(flat_ids - lax.axis_index("ep") + peers, peers)
    picked = back.reshape(peers * cap, width)[(shifted * cap + rank).reshape(rows, top)]
    routed = jnp.sum(picked.astype(F32) * route_weights[:, :, None], axis=1)
    result = (resid.astype(F32) + routed + dense_scale * dense_out.astype(F32)).astype(BF16)
    return result, new_state, new_conv


def solution(mesh):
    in_specs = (
        P("ep", "tp"),
        P("ep", None, "tp"),
        P("ep", "tp"),
        P(),
        P(None, "tp"),
        P(None, "tp"),
        P(None, "tp"),
        P("tp", None, None),
        P("tp", None, None),
        P("tp"),
        P(None, "tp"),
        P(),
        P("ep", None),
        P("ep", None),
        P("ep", None, "tp"),
        P("ep", None, "tp"),
        P("ep", None, "tp"),
        P(None, "tp"),
        P(None, "tp"),
        P(None, "tp"),
        P("tp"),
    )
    out_specs = (P("ep", "tp"), P("ep", "tp"), P("ep", None, "tp"))
    return jax.shard_map(
        per_device, mesh=mesh, in_specs=in_specs, out_specs=out_specs, check_vma=False
    )
```

```python
import functools

import jax
import jax.numpy as jnp
from jax import lax
from jax.experimental import pallas as pl
from jax.experimental.pallas import tpu as pltpu
from jax.sharding import PartitionSpec as P

BF16 = jnp.bfloat16
F32 = jnp.float32
VMEM = pl.BlockSpec(memory_space=pltpu.VMEM)
ANY = pl.BlockSpec(memory_space=pl.ANY)
HBM = pl.BlockSpec(memory_space=pltpu.HBM)


def dot(a, b):
    return jnp.dot(a, b, preferred_element_type=F32)


def remote(src, dst, send_sem, recv_sem, device):
    return pltpu.make_async_remote_copy(
        src_ref=src,
        dst_ref=dst,
        send_sem=send_sem,
        recv_sem=recv_sem,
        device_id=device,
        device_id_type=pl.DeviceIdType.MESH,
    )


def row_sums(rows):
    return (
        jnp.sum(rows, axis=1, keepdims=True),
        jnp.sum(rows * rows, axis=1, keepdims=True),
    )


def neg_expm1(y):
    series = 1.0 + y / 8.0
    for order in range(7, 1, -1):
        series = 1.0 + y / order * series
    return jnp.where(y > -0.3, -y * series, 1.0 - jnp.exp(y))


def norm_pair(own, own_sums, peer, gain_ref, t, out_ref):
    width = own.shape[1]
    peer_sums = row_sums(peer)
    mean = (own_sums[0] + peer_sums[0]) / (2 * width)
    var = (own_sums[1] + peer_sums[1]) / (2 * width) - mean * mean
    scale = lax.rsqrt(var + 1e-05)
    for slot, (rows, half) in enumerate(((own, t), (peer, 1 - t))):
        out_ref[slot] = ((rows - mean) * scale * gain_ref[half]).astype(BF16)


def mixer_kernel(
    stream_ref,
    part_ref,
    state_ref,
    gain_ref,
    branch_hbm,
    gate_hbm,
    taps_ref,
    rmap_ref,
    imap_ref,
    decay_ref,
    out_hbm,
    gain2_ref,
    branch_ref,
    new_state_ref,
    resid_ref,
    n2_ref,
    branch_w,
    gate_w,
    out_w,
    peer_ref,
    nrm_ref,
    mix_ref,
    res_ref,
    load_sem,
    send_sem,
    recv_sem,
):
    t = lax.axis_index("tp")
    partner = {"tp": 1 - t}
    loads = [
        pltpu.make_async_copy(src, dst, load_sem.at[i])
        for i, (src, dst) in enumerate(
            ((branch_hbm, branch_w), (gate_hbm, gate_w), (out_hbm, out_w))
        )
    ]
    for load in loads:
        load.start()
    barrier = pltpu.get_barrier_semaphore()
    pl.semaphore_signal(barrier, inc=1, device_id=partner, device_id_type=pl.DeviceIdType.MESH)
    pl.semaphore_wait(barrier, 1)
    first = remote(stream_ref, peer_ref, send_sem.at[0], recv_sem.at[0], partner)
    first.start()
    own = stream_ref[...].astype(F32)
    own_sums = row_sums(own)
    first.wait_recv()
    norm_pair(own, own_sums, peer_ref[...].astype(F32), gain_ref, t, nrm_ref)

    width = stream_ref.shape[1]
    block = rmap_ref.shape[1]
    chunk = 2 * block
    loads[0].wait()
    loads[1].wait()
    for c in range(width // chunk):
        cols = pl.ds(c * chunk, chunk)
        branch = dot(nrm_ref[0], branch_w[t, :, cols]) + dot(nrm_ref[1], branch_w[1 - t, :, cols])
        branch = branch.astype(BF16)
        branch_ref[:, cols] = branch
        gate = dot(nrm_ref[0], gate_w[t, :, cols]) + dot(nrm_ref[1], gate_w[1 - t, :, cols])
        gate = gate.astype(BF16).astype(F32)
        conv = (branch.astype(F32) * taps_ref[3:4, cols] + part_ref[:, cols]).astype(BF16)
        rec, inp = [], []
        for b in range(2):
            piece = conv[:, b * block : (b + 1) * block]
            rec.append(dot(piece, rmap_ref[2 * c + b]))
            inp.append(dot(piece, imap_ref[2 * c + b]))
        recur_gate = jax.nn.sigmoid(jnp.concatenate(rec, axis=1))
        input_gate = jax.nn.sigmoid(jnp.concatenate(inp, axis=1))
        logit = -decay_ref[:, cols]
        softplus = jnp.maximum(logit, 0.0) + jnp.log1p(jnp.exp(-jnp.abs(logit)))
        log_decay = -8.0 * recur_gate * softplus
        driven = jnp.sqrt(neg_expm1(2.0 * log_decay)) * (input_gate * conv.astype(F32))
        state = jnp.exp(log_decay) * state_ref[:, cols] + driven
        new_state_ref[:, cols] = state
        gelu = 0.5 * gate * (1.0 + jnp.tanh(0.7978845608028654 * (gate + 0.044715 * gate**3)))
        mix_ref[0, :, cols] = (gelu * state).astype(BF16)
    second = remote(mix_ref.at[0], mix_ref.at[1], send_sem.at[1], recv_sem.at[1], partner)
    second.start()
    loads[2].wait()
    mixed = dot(mix_ref[0], out_w[t])
    second.wait_recv()
    mixed = (mixed + dot(mix_ref[1], out_w[1 - t])).astype(BF16)
    resid = (own + mixed.astype(F32)).astype(BF16)
    res_ref[0] = resid
    third = remote(res_ref.at[0], res_ref.at[1], send_sem.at[2], recv_sem.at[2], partner)
    third.start()
    resid_ref[...] = resid
    resid = resid.astype(F32)
    sums = row_sums(resid)
    third.wait_recv()
    norm_pair(resid, sums, res_ref[1].astype(F32), gain2_ref, t, n2_ref)
    for copy in (first, second, third):
        copy.wait_send()


def flipped(q, r):
    return (q // 2 + r // 2) % 2 * 2 + (q + r) % 2


def layer_kernel(
    peers,
    stream_hbm,
    conv_hbm,
    state_hbm,
    gain_hbm,
    branch_hbm,
    gate_hbm,
    taps_hbm,
    rmap_hbm,
    imap_hbm,
    decay_hbm,
    out_hbm,
    gain2_hbm,
    ids_hbm,
    weights_hbm,
    scale_hbm,
    eg_hbm,
    eu_hbm,
    ed_hbm,
    dg_hbm,
    du_hbm,
    dd_hbm,
    result_hbm,
    new_state_hbm,
    new_conv_hbm,
    stream_ref,
    conv_ref,
    state_ref,
    gain_ref,
    branch_w,
    gate_w,
    taps_ref,
    rmap_ref,
    imap_ref,
    decay_ref,
    out_w,
    gain2_ref,
    ids_ref,
    weights_ref,
    scale_ref,
    eg,
    eu,
    ed,
    dg,
    du,
    dd,
    result_ref,
    new_state_ref,
    new_conv_ref,
    eg_peer,
    eu_peer,
    ed_peer,
    peer_ref,
    nrm_ref,
    mix_ref,
    res_ref,
    dhid,
    inc,
    snd,
    got_d,
    got_dz,
    got_x,
    got_y,
    zbuf,
    got_z,
    fin_x,
    fin_y,
    fin_o,
    base_ref,
    wsend,
    wrecv,
    load_sem,
    store_sem,
    m_send,
    m_recv,
    mix_send,
    mix_recv,
    e_send,
    e_recv,
    w_send,
    w_recv,
    link_send,
    link_recv,
    back_send,
    back_recv,
    fin_send,
    fin_recv,
    dz_send,
    dz_recv,
):
    e = lax.axis_index("ep")
    t = lax.axis_index("tp")
    partner = {"tp": 1 - t}
    depth = peers // 4
    z = e // 4
    q = e % 4
    x_near = 4 * z + flipped(q, 1)
    y_near = 4 * z + flipped(q, 2)
    rows, width = stream_ref.shape
    half = rows // 2
    mine = pl.ds(pl.multiple_of(half * t, half), half)
    pairs = (
        (stream_hbm, stream_ref),
        (gain_hbm, gain_ref),
        (branch_hbm, branch_w),
        (gate_hbm, gate_w),
        (conv_hbm, conv_ref),
        (taps_hbm, taps_ref),
        (rmap_hbm, rmap_ref),
        (imap_hbm, imap_ref),
        (decay_hbm, decay_ref),
        (state_hbm, state_ref),
        (out_hbm, out_w),
        (gain2_hbm, gain2_ref),
        (ids_hbm, ids_ref),
        (weights_hbm, weights_ref),
        (scale_hbm, scale_ref),
        (dg_hbm, dg),
        (du_hbm, du),
        (dd_hbm, dd),
        (eg_hbm, eg),
        (eu_hbm, eu),
        (ed_hbm, ed),
    )
    loads = [pltpu.make_async_copy(a, b, load_sem.at[i]) for i, (a, b) in enumerate(pairs)]
    for i in (0, 1, 12, 13, 2, 3, 4, 5, 6, 7, 8, 9):
        loads[i].start()
    barrier = pltpu.get_barrier_semaphore()
    pl.semaphore_signal(barrier, inc=1, device_id=partner, device_id_type=pl.DeviceIdType.MESH)

    @pl.loop(1, peers)
    def _(offset):
        for core in range(2):
            pl.semaphore_signal(
                barrier,
                inc=1,
                device_id={"ep": lax.rem(e + offset, peers), "tp": core},
                device_id_type=pl.DeviceIdType.MESH,
            )

    loads[0].wait()
    pl.semaphore_wait(barrier, 2 * peers - 1)
    first = remote(stream_ref, peer_ref, m_send.at[0], m_recv.at[0], partner)
    first.start()
    own = stream_ref[...].astype(F32)
    own_sums = row_sums(own)

    loads[12].wait()
    loads[13].wait()
    ids = ids_ref[...]
    weights = weights_ref[...]
    lanes = wsend.shape[2]
    for d in range(peers):
        row = jnp.sum(jnp.where(ids == d, weights, 0.0), axis=0, keepdims=True)
        wsend[d] = jnp.concatenate([row, jnp.zeros((1, lanes - rows), F32)], axis=1)

    def weighing(r, o):
        there = (z + o) % depth
        d = 4 * there + flipped(q, r)
        slot = 4 * z + r
        return remote(wsend.at[d], wrecv.at[slot], w_send.at[d], w_recv.at[slot], {"ep": d})

    places = [(r, o) for r in range(4) for o in range(depth) if r or o]
    for r, o in places:
        weighing(r, o).start()

    loads[1].wait()
    first.wait_recv()
    norm_pair(own, own_sums, peer_ref[...].astype(F32), gain_ref, t, nrm_ref)
    for load in loads[2:10]:
        load.wait()
    for i in (10, 11, 14, 15, 16, 17, 18, 19, 20):
        loads[i].start()
    pushes = [
        remote(a, b, e_send.at[i], e_recv.at[i], partner)
        for i, (a, b) in enumerate(((eg_hbm, eg_peer), (eu_hbm, eu_peer), (ed_hbm, ed_peer)))
    ]
    pushes[0].start()
    block = rmap_ref.shape[1]
    chunk = 2 * block
    for c in range(width // chunk):
        cols = pl.ds(c * chunk, chunk)
        branch = dot(nrm_ref[0], branch_w[t, :, cols]) + dot(nrm_ref[1], branch_w[1 - t, :, cols])
        branch = branch.astype(BF16)
        gate = dot(nrm_ref[0], gate_w[t, :, cols]) + dot(nrm_ref[1], gate_w[1 - t, :, cols])
        gate = gate.astype(BF16).astype(F32)
        conv = branch.astype(F32) * taps_ref[3:4, cols]
        for i in range(3):
            conv = conv + conv_ref[i, :, cols].astype(F32) * taps_ref[i : i + 1, cols]
        conv = conv.astype(BF16)
        new_conv_ref[0, :, cols] = conv_ref[1, :, cols]
        new_conv_ref[1, :, cols] = conv_ref[2, :, cols]
        new_conv_ref[2, :, cols] = branch
        rec, inp = [], []
        for b in range(2):
            piece = conv[:, b * block : (b + 1) * block]
            rec.append(dot(piece, rmap_ref[2 * c + b]))
            inp.append(dot(piece, imap_ref[2 * c + b]))
        recur_gate = jax.nn.sigmoid(jnp.concatenate(rec, axis=1))
        input_gate = jax.nn.sigmoid(jnp.concatenate(inp, axis=1))
        logit = -decay_ref[:, cols]
        softplus = jnp.maximum(logit, 0.0) + jnp.log1p(jnp.exp(-jnp.abs(logit)))
        log_decay = -8.0 * recur_gate * softplus
        driven = jnp.sqrt(neg_expm1(2.0 * log_decay)) * (input_gate * conv.astype(F32))
        state = jnp.exp(log_decay) * state_ref[:, cols] + driven
        new_state_ref[:, cols] = state
        gelu = 0.5 * gate * (1.0 + jnp.tanh(0.7978845608028654 * (gate + 0.044715 * gate**3)))
        mix_ref[0, :, cols] = (gelu * state).astype(BF16)
    second = remote(mix_ref.at[0], mix_ref.at[1], mix_send.at[0], mix_recv.at[0], partner)
    second.start()
    stores = [
        pltpu.make_async_copy(new_state_ref, new_state_hbm, store_sem.at[0]),
        pltpu.make_async_copy(new_conv_ref, new_conv_hbm, store_sem.at[1]),
    ]
    for store in stores:
        store.start()
    loads[10].wait()
    mixed = dot(mix_ref[0], out_w[t])
    second.wait_recv()
    mixed = (mixed + dot(mix_ref[1], out_w[1 - t])).astype(BF16)
    resid = (own + mixed.astype(F32)).astype(BF16)
    res_ref[0] = resid
    third = remote(res_ref.at[0], res_ref.at[1], m_send.at[1], m_recv.at[1], partner)
    third.start()
    resid = resid.astype(F32)
    sums = row_sums(resid)
    loads[11].wait()
    third.wait_recv()
    norm_pair(resid, sums, res_ref[1].astype(F32), gain2_ref, t, nrm_ref)
    inc[4 * z, t] = nrm_ref[0, mine, :]
    inc[4 * z, 1 - t] = nrm_ref[1, mine, :]

    turn = 1 + z // 2 * 2
    mid = (z % 3 + 1) // 2
    o_b = 2 + mid
    o_c = 3 - mid

    def at(o):
        return (z + o * turn) % depth

    def z_copy(o, h):
        here = inc.at[4 * z, h]
        there = {"ep": 4 * at(o) + q}
        return remote(here, here, link_send.at[0, o, h], link_recv.at[0, z, h], there)

    def z_relay(o, h):
        j = at(o)
        here = inc.at[4 * j, h]
        there = {"ep": 4 * at(4 - o) + q}
        return remote(here, here, dz_send.at[2, o - 1, h], link_recv.at[0, j, h], there)

    def z_wait(o, h):
        j = at(o)
        here = inc.at[4 * j, h]
        remote(here, here, link_send.at[0, j, h], link_recv.at[0, j, h], partner).wait_recv()

    def side_copy(r, o, h):
        j = at(o)
        return remote(
            inc.at[4 * j, h],
            inc.at[4 * j + r, h],
            link_send.at[r, j, h],
            link_recv.at[r, j, h],
            {"ep": x_near if r == 1 else y_near},
        )

    def d_copy(h, o):
        j = at(o)
        return remote(
            inc.at[4 * j + 1 + h, h],
            inc.at[4 * j + 3, h],
            link_send.at[3, j, h],
            link_recv.at[3, j, h],
            {"ep": x_near if h else y_near},
        )

    def sides(o):
        side_copy(1, o, 0).start()
        side_copy(2, o, 1).start()
        side_copy(1, o, 1).start()
        side_copy(2, o, 0).start()

    def along(o):
        z_wait(o, 0)
        if o != 2:

            @pl.when(mid == 1)
            def _():
                z_relay(o, 0).start()

        side_copy(1, o, 0).start()
        z_wait(o, 1)
        if o != 2:

            @pl.when(mid == 1)
            def _():
                z_relay(o, 1).start()

        side_copy(2, o, 1).start()
        side_copy(1, o, 1).start()
        side_copy(2, o, 0).start()

    def dz_copy(o, h):
        here = inc.at[4 * z + 3, h]
        there = {"ep": 4 * at(o) + q}
        return remote(here, here, dz_send.at[0, o, h], link_recv.at[3, z, h], there)

    def dz_relay(o, h):
        j = at(o)
        here = inc.at[4 * j + 3, h]
        there = {"ep": 4 * at(4 - o) + q}
        return remote(here, here, dz_send.at[1, o, h], link_recv.at[3, j, h], there)

    def dz():
        for h in range(2):
            d_copy(h, 0).wait_recv()
            dz_copy(1, h).start()

            @pl.when(mid == 1)
            def _():
                dz_copy(3, h).start()

    def dzr():
        @pl.when(mid == 1)
        def _():
            for h in range(2):
                d_copy(h, 1).wait_recv()
                dz_relay(1, h).start()

    def near(o):
        for h in range(2):
            side_copy(1 + h, o, h).wait_recv()
            d_copy(h, o).start()

    def near_sides(o):
        side_copy(1, o, 0).wait_recv()
        side_copy(2, o, 1).wait_recv()

    spread = lax.broadcasted_iota(jnp.int32, (half, lanes), 0) + half * t == (
        lax.broadcasted_iota(jnp.int32, (half, lanes), 1)
    )

    def arrived_sides(o):
        side_copy(1, o, 1).wait_recv()
        side_copy(2, o, 0).wait_recv()

    def arrived(o):
        arrived_sides(o)
        if not (isinstance(o, int) and o == 0):
            for h in range(2):
                d_copy(h, o).wait_recv()

    def arr_end(o):
        arrived_sides(o)

        @pl.when(mid == 0)
        def _():
            for h in range(2):
                d_copy(h, o).wait_recv()

    def serve(o):
        slot = 4 * at(o)
        part = pl.ds(slot, 4)
        cols = []
        for r in range(4):
            cols.append(jnp.sum(jnp.where(spread, wrecv[slot + r], 0.0), axis=1, keepdims=True))
        scale = jnp.concatenate(cols, axis=0)
        low = inc[part, 0].reshape(4 * half, width)
        high = inc[part, 1].reshape(4 * half, width)
        hidden = []
        for gate_e, up_e in ((eg, eu), (eg_peer, eu_peer)):
            gate = dot(low, gate_e[0]) + dot(high, gate_e[1])
            up = dot(low, up_e[0]) + dot(high, up_e[1])
            hidden.append((jax.nn.silu(gate) * up).astype(BF16))
        for h, down in ((t, ed), (1 - t, ed_peer)):
            served = (dot(hidden[0], down[t]) + dot(hidden[1], down[1 - t])) * scale
            snd[part, h] = served.astype(BF16).reshape(4, half, width)

    def d_back(h, o):
        j = at(o)
        return remote(
            snd.at[4 * j + 3, h],
            got_d.at[j, h],
            back_send.at[3, j, h],
            back_recv.at[3, j, h],
            {"ep": x_near if h else y_near},
        )

    def side_back(r, o, h):
        j = at(o)
        near_chip = x_near if r == 1 else y_near
        if isinstance(o, int) and o == 0:
            return remote(
                snd.at[4 * j + r, h],
                (fin_x if r == 1 else fin_y).at[mine],
                back_send.at[r, j, h],
                fin_recv.at[r, t],
                {"ep": near_chip, "tp": h},
            )
        return remote(
            snd.at[4 * j + r, h],
            (got_x if r == 1 else got_y).at[j, h],
            back_send.at[r, j, h],
            back_recv.at[r, j, h],
            {"ep": near_chip},
        )

    def dz_back(o, h):
        j = at(o)
        there = {"ep": 4 * j + q}
        return remote(
            snd.at[4 * j + 3, h], got_dz.at[z, h], dz_send.at[3, o, h], dz_recv.at[z, h], there
        )

    def dz_pass(h):
        j = at(2)
        there = {"ep": 4 * at(1) + q}
        return remote(
            snd.at[4 * j + 3, h], got_d.at[j, h], dz_send.at[3, 2, h], back_recv.at[3, j, h], there
        )

    def merge(slot, h, *parts):
        total = snd[slot, h].astype(F32)
        for part in parts:
            total = total + part.astype(F32)
        snd[slot, h] = total.astype(BF16)

    def send_all(o):
        for h in range(2):
            side_back(1, o, h).start()
            side_back(2, o, 1 - h).start()

    def send_first(o):
        d_back(0, o).start()
        d_back(1, o).start()
        side_back(1, o, 1).start()
        side_back(2, o, 0).start()

    def joined(o):
        j = at(o)
        for h in range(2):
            d_back(h, o).wait_recv()
            merge(4 * j + 1 + h, h, got_d[j, h])
            side_back(1 + h, o, h).start()

    def passed(o):
        j = at(o)
        for h in range(2):
            d_back(h, o).wait_recv()
            merge(4 * j + 3, h, got_d[j, h])
            dz_back(o, h).start()

    def dz_wait(o, h):
        j = at(o)
        here = got_dz.at[j, h]
        remote(here, here, dz_send.at[3, o, h], dz_recv.at[j, h], partner).wait_recv()

    def send_own():
        @pl.when(mid == 1)
        def _():
            for h in range(2):
                dz_wait(3, h)
                merge(4 * z + 3, h, got_dz[at(3), h])

        for h in range(2):
            dz_wait(1, h)
            merge(4 * z + 3, h, got_dz[at(1), h])
            d_back(h, 0).start()

    def bz_copy(o, h):
        j = at(o)
        return remote(
            zbuf.at[j, h],
            got_z.at[z, mine],
            back_send.at[0, j, h],
            back_recv.at[0, z, t],
            {"ep": 4 * j + q, "tp": h},
        )

    def bz_wait(o, core):
        j = at(o)
        here = got_z.at[j, pl.ds(core * half, half)]
        remote(here, here, back_send.at[0, j, 0], back_recv.at[0, j, core], partner).wait_recv()

    def home(o):
        j = at(o)
        for h in range(2):
            side_back(1, o, h).wait_recv()
            side_back(2, o, h).wait_recv()
            total = snd[4 * j, h].astype(F32) + got_x[j, h].astype(F32) + got_y[j, h].astype(F32)
            zbuf[j, h] = total.astype(BF16)
            bz_copy(o, h).start()

    own_copy = remote(snd.at[4 * z, 1 - t], fin_o, fin_send.at[0], fin_recv.at[0, 0], partner)

    for o in (1, 3):
        for h in range(2):
            z_copy(o, h).start()
    sides(0)
    pushes[1].start()
    pushes[2].start()

    for load in loads[14:18]:
        load.wait()
    dense_gate = dot(nrm_ref[0], dg[t]) + dot(nrm_ref[1], dg[1 - t])
    dense_up = dot(nrm_ref[0], du[t]) + dot(nrm_ref[1], du[1 - t])
    dhid[0] = (jax.nn.silu(dense_gate) * dense_up).astype(BF16)
    dense_copy = remote(dhid.at[0], dhid.at[1], m_send.at[2], m_recv.at[2], partner)
    dense_copy.start()
    near(0)
    along(1)
    for r, o in places:
        slot = 4 * ((z + o) % depth) + r
        remote(wsend.at[0], wrecv.at[slot], w_send.at[0], w_recv.at[slot], partner).wait_recv()
    row = jnp.sum(jnp.where(ids == e, weights, 0.0), axis=0, keepdims=True)
    wrecv[4 * z] = jnp.concatenate([row, jnp.zeros((1, lanes - rows), F32)], axis=1)
    dense = dot(dhid[0], dd[t])
    dense_copy.wait_recv()
    dense = (dense + dot(dhid[1], dd[1 - t])).astype(BF16)
    base_ref[...] = resid + scale_ref[...] * dense.astype(F32)
    for load in loads[18:]:
        load.wait()
    for push in pushes:
        push.wait_recv()
    along(3)
    dz()
    along(2)
    arrived(0)
    serve(0)
    own_copy.start()
    near(o_c)
    dzr()
    near_sides(1)
    arr_end(1)
    serve(1)
    send_all(1)

    @pl.when(mid == 0)
    def _():
        dz_back(1, 0).start()
        dz_back(1, 1).start()

    near_sides(o_b)
    arrived(o_b)
    serve(o_b)

    @pl.when(mid == 0)
    def _():
        dz_pass(0).start()
        dz_pass(1).start()


    @pl.when(mid == 1)
    def _():
        dz_back(3, 0).start()
        dz_back(3, 1).start()

    send_all(o_b)
    arrived(o_c)
    serve(o_c)
    send_first(o_c)
    home(1)

    @pl.when(mid == 1)
    def _():
        passed(1)

    joined(o_c)
    side_back(1, 0, 1).start()
    side_back(2, 0, 0).start()
    home(o_b)
    home(o_c)
    send_own()
    joined(0)
    other = pl.ds(pl.multiple_of(half - half * t, half), half)
    base_ref[mine, :] += snd[4 * z, t].astype(F32)
    own_copy.wait_recv()
    base_ref[other, :] += fin_o[...].astype(F32)
    total = base_ref[...]
    for o in range(1, depth):
        for core in range(2):
            bz_wait(o, core)
        total = total + got_z[at(o)].astype(F32)
    for r, fin in ((1, fin_x), (2, fin_y)):
        for core in range(2):
            here = fin.at[pl.ds(core * half, half)]
            remote(here, here, fin_send.at[1], fin_recv.at[r, core], partner).wait_recv()
        total = total + fin[...].astype(F32)
    result_ref[...] = total.astype(BF16)
    stores.append(pltpu.make_async_copy(result_ref, result_hbm, store_sem.at[2]))
    stores[-1].start()
    for copy in (first, third, dense_copy, own_copy, second, *pushes):
        copy.wait_send()
    for r, o in places:
        weighing(r, o).wait_send()
    for o in range(depth):
        for h in range(2):
            if o:
                bz_copy(o, h).wait_send()
            if o in (1, 3):
                z_copy(o, h).wait_send()
            for r in (1, 2):
                side_copy(r, o, h).wait_send()
                side_back(r, o, h).wait_send()
        if o == 0:
            for h in range(2):
                d_copy(h, o).wait_send()
                d_back(h, o).wait_send()

    @pl.when(mid == 1)
    def _():
        for h in range(2):
            z_relay(1, h).wait_send()
            z_relay(3, h).wait_send()
            dz_relay(1, h).wait_send()
            dz_copy(3, h).wait_send()
            dz_back(3, h).wait_send()

    @pl.when(mid == 0)
    def _():
        for h in range(2):
            dz_pass(h).wait_send()

    for h in range(2):
        d_copy(h, o_c).wait_send()
        d_back(h, o_c).wait_send()
        dz_copy(1, h).wait_send()
        dz_back(1, h).wait_send()

    for store in stores:
        store.wait()


def expert_kernel(
    full,
    peers,
    group,
    n2_ref,
    out_ref,
    resid_ref,
    ids_ref,
    weights_ref,
    scale_ref,
    eg_hbm,
    eu_hbm,
    ed_hbm,
    dg_hbm,
    du_hbm,
    dd_hbm,
    *refs,
):
    if full:
        result_ref, *refs = refs
    else:
        dense_ref, back_ref, *refs = refs
    (
        eg,
        eu,
        ed,
        dg,
        du,
        dd,
        inc,
        hid,
        src,
        ret,
        dhid,
        load_sem,
        own_sem,
        x_send,
        x_recv,
        f_send,
        f_recv,
        h_send,
        h_recv,
        r_send,
        r_recv,
        d_sem,
    ) = refs
    e = lax.axis_index("ep")
    t = lax.axis_index("tp")
    partner = {"tp": 1 - t}
    groups = peers // group
    cap = inc.shape[2]
    width = inc.shape[3]
    loads = [
        pltpu.make_async_copy(a, b, load_sem.at[i])
        for i, (a, b) in enumerate(
            ((dg_hbm, dg), (du_hbm, du), (dd_hbm, dd), (eg_hbm, eg), (eu_hbm, eu), (ed_hbm, ed))
        )
    ]
    for load in loads:
        load.start()

    def outgoing(offset):
        return n2_ref.at[0] if full else out_ref.at[lax.rem(e + offset, peers)]

    keep = pltpu.make_async_copy(outgoing(0), inc.at[0, 0], own_sem)
    keep.start()
    barrier = pltpu.get_barrier_semaphore()
    pl.semaphore_signal(barrier, inc=1, device_id=partner, device_id_type=pl.DeviceIdType.MESH)

    @pl.loop(1, peers)
    def _(offset):
        pl.semaphore_signal(
            barrier,
            inc=1,
            device_id={"ep": lax.rem(e + offset, peers)},
            device_id_type=pl.DeviceIdType.MESH,
        )

    pl.semaphore_wait(barrier, peers)

    def sending(offset):
        return remote(
            outgoing(offset),
            inc.at[0, offset],
            x_send.at[offset],
            x_recv.at[offset],
            {"ep": lax.rem(e + offset, peers)},
        )

    @pl.loop(1, peers)
    def _(offset):
        sending(offset).start()

    for load in loads[:3]:
        load.wait()
    rows0, rows1 = n2_ref[0], n2_ref[1]
    dense_gate = dot(rows0, dg[t]) + dot(rows1, dg[1 - t])
    dense_up = dot(rows0, du[t]) + dot(rows1, du[1 - t])
    dhid[0] = (jax.nn.silu(dense_gate) * dense_up).astype(BF16)
    dense_copy = remote(dhid.at[0], dhid.at[1], d_sem.at[0], d_sem.at[1], partner)
    dense_copy.start()
    dense = dot(dhid[0], dd[t])
    dense_copy.wait()
    dense = (dense + dot(dhid[1], dd[1 - t])).astype(BF16)
    keep.wait()
    for load in loads[3:]:
        load.wait()

    def forwarding(g):
        part = pl.ds(g * group, group)
        return remote(inc.at[0, part], inc.at[1, part], f_send.at[g], f_recv.at[g], partner)

    def hiding(g):
        part = pl.ds(g * group, group)
        return remote(hid.at[0, part], hid.at[1, part], h_send.at[g], h_recv.at[g], partner)

    def returning(offset):
        return remote(
            src.at[offset],
            ret.at[offset],
            r_send.at[offset],
            r_recv.at[offset],
            {"ep": lax.rem(e + peers - offset, peers)},
        )

    def arrive(g):
        @pl.loop(max(1, g * group), (g + 1) * group)
        def _(offset):
            sending(offset).wait_recv()

        forwarding(g).start()

    def upward(g):
        forwarding(g).wait_recv()
        part = pl.ds(g * group, group)
        own = inc[0, part].reshape(group * cap, width)
        peer = inc[1, part].reshape(group * cap, width)
        gate = dot(own, eg[t]) + dot(peer, eg[1 - t])
        up = dot(own, eu[t]) + dot(peer, eu[1 - t])
        hidden = (jax.nn.silu(gate) * up).astype(BF16)
        hid[0, part] = hidden.reshape(group, cap, -1)
        hiding(g).start()

    def downward(g):
        hiding(g).wait_recv()
        part = pl.ds(g * group, group)
        own = hid[0, part].reshape(group * cap, -1)
        peer = hid[1, part].reshape(group * cap, -1)
        served = dot(own, ed[t]) + dot(peer, ed[1 - t])
        src[part] = served.astype(BF16).reshape(group, cap, width)

        @pl.loop(max(1, g * group), (g + 1) * group)
        def _(offset):
            returning(offset).start()

    for step in range(groups + 2):
        if step < groups:
            arrive(step)
        if 1 <= step <= groups:
            upward(step - 1)
        if step >= 2:
            downward(step - 2)

    if full:
        total = resid_ref[...].astype(F32) + scale_ref[...] * dense.astype(F32)
        ids = ids_ref[...]
        weights = weights_ref[...]

        def weight(offset):
            chosen = ids == lax.rem(e + offset, peers)
            return jnp.sum(jnp.where(chosen, weights, 0.0), axis=1, keepdims=True)

        routed = weight(0) * src[0].astype(F32)
        for offset in range(1, peers):
            returning(offset).wait_recv()
            routed = routed + weight(offset) * ret[offset].astype(F32)
        result_ref[...] = (total + routed).astype(BF16)
    else:
        dense_ref[...] = dense
        back_ref[0] = src[0]

        @pl.loop(1, peers)
        def _(offset):
            returning(offset).wait_recv()
            back_ref[offset] = ret[offset]

    @pl.loop(1, peers)
    def _(offset):
        sending(offset).wait_send()
        returning(offset).wait_send()

    @pl.loop(0, groups)
    def _(g):
        forwarding(g).wait_send()
        hiding(g).wait_send()


def emit_kernel(a_in, b_in, c_in, a_out, b_out, c_out, a, b, c, sem):
    sets = tuple(enumerate(((a_in, a, a_out), (b_in, b, b_out), (c_in, c, c_out))))
    reads = [pltpu.make_async_copy(src, mid, sem.at[0, i]) for i, (src, mid, _) in sets]
    writes = [pltpu.make_async_copy(mid, dst, sem.at[1, i]) for i, (_, mid, dst) in sets]
    for read in reads:
        read.start()
    for read, write in zip(reads, writes):
        read.wait()
        write.start()
    for write in writes:
        write.wait()


def halves(weight):
    return weight.reshape(2, weight.shape[0] // 2, weight.shape[1])


def per_device(
    stream,
    conv_state,
    recur_state,
    mix_gain,
    branch_weight,
    gate_weight,
    conv_taps,
    recur_map,
    input_map,
    decay_logit,
    out_weight,
    moe_gain,
    route_ids,
    route_weights,
    expert_gate,
    expert_up,
    expert_down,
    dense_gate,
    dense_up,
    dense_down,
    dense_scale,
):
    rows, width = stream.shape
    dma = pltpu.SemaphoreType.DMA
    top = route_ids.shape[1]
    peers = lax.axis_size("ep")
    cap = max(2, min(rows, 3 * rows * top // peers))
    if cap == rows and peers // 4 == 4:
        operands = (
            stream,
            conv_state.transpose(1, 0, 2),
            recur_state,
            mix_gain.reshape(2, 1, width),
            halves(branch_weight),
            halves(gate_weight),
            conv_taps,
            recur_map,
            input_map,
            decay_logit.reshape(1, width),
            halves(out_weight),
            moe_gain.reshape(2, 1, width),
            route_ids.T,
            route_weights.T,
            dense_scale.reshape(1, width),
            halves(expert_gate[0]),
            halves(expert_up[0]),
            halves(expert_down[0]),
            halves(dense_gate),
            halves(dense_up),
            halves(dense_down),
        )
        depth = peers // 4
        half = rows // 2
        lanes = -(-rows // 128) * 128
        outs = (
            jax.ShapeDtypeStruct((rows, width), BF16),
            jax.ShapeDtypeStruct((rows, width), F32),
            jax.ShapeDtypeStruct((3, rows, width), BF16),
        )
        column = pltpu.VMEM((depth, 2, half, width), BF16)
        whole = pltpu.VMEM((rows, width), BF16)
        result, new_state, new_conv = pl.pallas_call(
            functools.partial(layer_kernel, peers),
            out_shape=outs,
            in_specs=[ANY] * len(operands),
            out_specs=[ANY] * 3,
            scratch_shapes=[pltpu.VMEM(a.shape, a.dtype) for a in operands + outs + operands[15:18]]
            + [whole]
            + [pltpu.VMEM((2, rows, width), BF16)] * 3
            + [pltpu.VMEM((2, rows, dense_gate.shape[1]), BF16)]
            + [pltpu.VMEM((peers, 2, half, width), BF16)] * 2
            + [column] * 5
            + [pltpu.VMEM((depth, rows, width), BF16)]
            + [whole] * 2
            + [pltpu.VMEM((half, width), BF16), pltpu.VMEM((rows, width), F32)]
            + [pltpu.VMEM((peers, 1, lanes), F32)] * 2
            + [dma((len(operands),)), dma((3,))]
            + [dma((3,))] * 2
            + [dma((1,))] * 2
            + [dma((3,))] * 2
            + [dma((peers,))] * 2
            + [dma((4, depth, 2))] * 4
            + [dma((2,)), dma((3, 2)), dma((4, depth, 2)), dma((depth, 2))],
            compiler_params=pltpu.CompilerParams(
                collective_id=2, has_side_effects=True, vmem_limit_bytes=63 * 1024 * 1024
            ),
            name="layer",
        )(*operands)
        result, new_state, new_conv = pl.pallas_call(
            emit_kernel,
            out_shape=tuple(jax.ShapeDtypeStruct(a.shape, a.dtype) for a in (result, new_state, new_conv)),
            in_specs=[ANY] * 3,
            out_specs=[ANY] * 3,
            scratch_shapes=[pltpu.VMEM(a.shape, a.dtype) for a in (result, new_state, new_conv)]
            + [dma((2, 3))],
            compiler_params=pltpu.CompilerParams(vmem_limit_bytes=63 * 1024 * 1024),
            name="emit",
        )(result, new_state, new_conv)
        return result, new_state, new_conv.transpose(1, 0, 2)
    conv_part = sum(conv_state[:, i].astype(F32) * conv_taps[i] for i in range(3))
    branch_in, new_state, resid, n2 = pl.pallas_call(
        mixer_kernel,
        out_shape=(
            jax.ShapeDtypeStruct((rows, width), BF16),
            jax.ShapeDtypeStruct((rows, width), F32),
            jax.ShapeDtypeStruct((rows, width), BF16),
            jax.ShapeDtypeStruct((2, rows, width), BF16),
        ),
        in_specs=[VMEM] * 4 + [ANY] * 2 + [VMEM] * 4 + [ANY, VMEM],
        out_specs=[VMEM] * 4,
        scratch_shapes=[pltpu.VMEM((2, width, width), BF16)] * 3
        + [pltpu.VMEM((rows, width), BF16)]
        + [pltpu.VMEM((2, rows, width), BF16)] * 3
        + [dma((3,))] * 3,
        compiler_params=pltpu.CompilerParams(
            collective_id=0, has_side_effects=True, vmem_limit_bytes=48 * 1024 * 1024
        ),
        name="mixer",
    )(
        stream,
        conv_part,
        recur_state,
        mix_gain.reshape(2, 1, width),
        halves(branch_weight),
        halves(gate_weight),
        conv_taps,
        recur_map,
        input_map,
        decay_logit.reshape(1, width),
        halves(out_weight),
        moe_gain.reshape(2, 1, width),
    )
    new_conv = jnp.concatenate([conv_state[:, 1:], branch_in[:, None]], axis=1)

    full = cap == rows
    if full:
        outgoing = jnp.zeros((8, 128), BF16)
    else:
        cap = -(-cap // 16) * 16
        flat_ids = route_ids.reshape(-1)
        one_hot = (flat_ids[:, None] == jnp.arange(peers, dtype=jnp.int32)[None, :]).astype(jnp.int32)
        rank = jnp.sum(one_hot * (jnp.cumsum(one_hot, axis=0) - 1), axis=1)
        slots = (flat_ids * cap + rank).reshape(rows, top)
        table = jnp.sum(
            (slots[:, :, None] == jnp.arange(peers * cap, dtype=jnp.int32)).astype(BF16), axis=1
        )
        outgoing = lax.dot_general(
            table, n2[0], (((0,), (0,)), ((), ())), preferred_element_type=F32
        )
        outgoing = outgoing.astype(BF16).reshape(peers, cap, width)
    group = max(1, min(peers, 256 // cap))
    while peers % group:
        group -= 1
    groups = peers // group
    hidden = expert_gate.shape[2]
    out_shape = [jax.ShapeDtypeStruct((rows, width), BF16)]
    if not full:
        out_shape.append(jax.ShapeDtypeStruct((peers, cap, width), BF16))
    outs = pl.pallas_call(
        functools.partial(expert_kernel, full, peers, group),
        out_shape=out_shape,
        in_specs=[VMEM] * 6 + [ANY] * 6,
        out_specs=[VMEM] * len(out_shape),
        scratch_shapes=[
            pltpu.VMEM((2, width, hidden), BF16),
            pltpu.VMEM((2, width, hidden), BF16),
            pltpu.VMEM((2, hidden, width), BF16),
            pltpu.VMEM((2, width, dense_gate.shape[1]), BF16),
            pltpu.VMEM((2, width, dense_gate.shape[1]), BF16),
            pltpu.VMEM((2, dense_gate.shape[1], width), BF16),
            pltpu.VMEM((2, peers, cap, width), BF16),
            pltpu.VMEM((2, peers, cap, hidden), BF16),
            pltpu.VMEM((peers, cap, width), BF16),
            pltpu.VMEM((peers, cap, width), BF16),
            pltpu.VMEM((2, rows, dense_gate.shape[1]), BF16),
            dma((6,)),
            dma,
            dma((peers,)),
            dma((peers,)),
            dma((groups,)),
            dma((groups,)),
            dma((groups,)),
            dma((groups,)),
            dma((peers,)),
            dma((peers,)),
            dma((2,)),
        ],
        compiler_params=pltpu.CompilerParams(
            collective_id=1, has_side_effects=True, vmem_limit_bytes=56 * 1024 * 1024
        ),
        name="experts",
    )(
        n2,
        outgoing,
        resid,
        route_ids,
        route_weights,
        dense_scale.reshape(1, width),
        halves(expert_gate[0]),
        halves(expert_up[0]),
        halves(expert_down[0]),
        halves(dense_gate),
        halves(dense_up),
        halves(dense_down),
    )
    if full:
        return outs[0], new_state, new_conv
    dense_out, back = outs
    shifted = lax.rem(flat_ids - lax.axis_index("ep") + peers, peers)
    picked = back.reshape(peers * cap, width)[(shifted * cap + rank).reshape(rows, top)]
    routed = jnp.sum(picked.astype(F32) * route_weights[:, :, None], axis=1)
    result = (resid.astype(F32) + routed + dense_scale * dense_out.astype(F32)).astype(BF16)
    return result, new_state, new_conv


def solution(mesh):
    in_specs = (
        P("ep", "tp"),
        P("ep", None, "tp"),
        P("ep", "tp"),
        P(),
        P(None, "tp"),
        P(None, "tp"),
        P(None, "tp"),
        P("tp", None, None),
        P("tp", None, None),
        P("tp"),
        P(None, "tp"),
        P(),
        P("ep", None),
        P("ep", None),
        P("ep", None, "tp"),
        P("ep", None, "tp"),
        P("ep", None, "tp"),
        P(None, "tp"),
        P(None, "tp"),
        P(None, "tp"),
        P("tp"),
    )
    out_specs = (P("ep", "tp"), P("ep", "tp"), P("ep", None, "tp"))
    return jax.shard_map(
        per_device, mesh=mesh, in_specs=in_specs, out_specs=out_specs, check_vma=False
    )
```

```python
import functools

import jax
import jax.numpy as jnp
from jax import lax
from jax.experimental import pallas as pl
from jax.experimental.pallas import tpu as pltpu
from jax.sharding import PartitionSpec as P

BF16 = jnp.bfloat16
F32 = jnp.float32
VMEM = pl.BlockSpec(memory_space=pltpu.VMEM)
ANY = pl.BlockSpec(memory_space=pl.ANY)
HBM = pl.BlockSpec(memory_space=pltpu.HBM)


def dot(a, b):
    return jnp.dot(a, b, preferred_element_type=F32)


def remote(src, dst, send_sem, recv_sem, device):
    return pltpu.make_async_remote_copy(
        src_ref=src,
        dst_ref=dst,
        send_sem=send_sem,
        recv_sem=recv_sem,
        device_id=device,
        device_id_type=pl.DeviceIdType.MESH,
    )


def row_sums(rows):
    return (
        jnp.sum(rows, axis=1, keepdims=True),
        jnp.sum(rows * rows, axis=1, keepdims=True),
    )


def neg_expm1(y):
    series = 1.0 + y / 8.0
    for order in range(7, 1, -1):
        series = 1.0 + y / order * series
    return jnp.where(y > -0.3, -y * series, 1.0 - jnp.exp(y))


def norm_pair(own, own_sums, peer, gain_ref, t, out_ref):
    width = own.shape[1]
    peer_sums = row_sums(peer)
    mean = (own_sums[0] + peer_sums[0]) / (2 * width)
    var = (own_sums[1] + peer_sums[1]) / (2 * width) - mean * mean
    scale = lax.rsqrt(var + 1e-05)
    for slot, (rows, half) in enumerate(((own, t), (peer, 1 - t))):
        out_ref[slot] = ((rows - mean) * scale * gain_ref[half]).astype(BF16)


def mixer_kernel(
    stream_ref,
    part_ref,
    state_ref,
    gain_ref,
    branch_hbm,
    gate_hbm,
    taps_ref,
    rmap_ref,
    imap_ref,
    decay_ref,
    out_hbm,
    gain2_ref,
    branch_ref,
    new_state_ref,
    resid_ref,
    n2_ref,
    branch_w,
    gate_w,
    out_w,
    peer_ref,
    nrm_ref,
    mix_ref,
    res_ref,
    load_sem,
    send_sem,
    recv_sem,
):
    t = lax.axis_index("tp")
    partner = {"tp": 1 - t}
    loads = [
        pltpu.make_async_copy(src, dst, load_sem.at[i])
        for i, (src, dst) in enumerate(
            ((branch_hbm, branch_w), (gate_hbm, gate_w), (out_hbm, out_w))
        )
    ]
    for load in loads:
        load.start()
    barrier = pltpu.get_barrier_semaphore()
    pl.semaphore_signal(barrier, inc=1, device_id=partner, device_id_type=pl.DeviceIdType.MESH)
    pl.semaphore_wait(barrier, 1)
    first = remote(stream_ref, peer_ref, send_sem.at[0], recv_sem.at[0], partner)
    first.start()
    own = stream_ref[...].astype(F32)
    own_sums = row_sums(own)
    first.wait_recv()
    norm_pair(own, own_sums, peer_ref[...].astype(F32), gain_ref, t, nrm_ref)

    width = stream_ref.shape[1]
    block = rmap_ref.shape[1]
    chunk = 2 * block
    loads[0].wait()
    loads[1].wait()
    for c in range(width // chunk):
        cols = pl.ds(c * chunk, chunk)
        branch = dot(nrm_ref[0], branch_w[t, :, cols]) + dot(nrm_ref[1], branch_w[1 - t, :, cols])
        branch = branch.astype(BF16)
        branch_ref[:, cols] = branch
        gate = dot(nrm_ref[0], gate_w[t, :, cols]) + dot(nrm_ref[1], gate_w[1 - t, :, cols])
        gate = gate.astype(BF16).astype(F32)
        conv = (branch.astype(F32) * taps_ref[3:4, cols] + part_ref[:, cols]).astype(BF16)
        rec, inp = [], []
        for b in range(2):
            piece = conv[:, b * block : (b + 1) * block]
            rec.append(dot(piece, rmap_ref[2 * c + b]))
            inp.append(dot(piece, imap_ref[2 * c + b]))
        recur_gate = jax.nn.sigmoid(jnp.concatenate(rec, axis=1))
        input_gate = jax.nn.sigmoid(jnp.concatenate(inp, axis=1))
        logit = -decay_ref[:, cols]
        softplus = jnp.maximum(logit, 0.0) + jnp.log1p(jnp.exp(-jnp.abs(logit)))
        log_decay = -8.0 * recur_gate * softplus
        driven = jnp.sqrt(neg_expm1(2.0 * log_decay)) * (input_gate * conv.astype(F32))
        state = jnp.exp(log_decay) * state_ref[:, cols] + driven
        new_state_ref[:, cols] = state
        gelu = 0.5 * gate * (1.0 + jnp.tanh(0.7978845608028654 * (gate + 0.044715 * gate**3)))
        mix_ref[0, :, cols] = (gelu * state).astype(BF16)
    second = remote(mix_ref.at[0], mix_ref.at[1], send_sem.at[1], recv_sem.at[1], partner)
    second.start()
    loads[2].wait()
    mixed = dot(mix_ref[0], out_w[t])
    second.wait_recv()
    mixed = (mixed + dot(mix_ref[1], out_w[1 - t])).astype(BF16)
    resid = (own + mixed.astype(F32)).astype(BF16)
    res_ref[0] = resid
    third = remote(res_ref.at[0], res_ref.at[1], send_sem.at[2], recv_sem.at[2], partner)
    third.start()
    resid_ref[...] = resid
    resid = resid.astype(F32)
    sums = row_sums(resid)
    third.wait_recv()
    norm_pair(resid, sums, res_ref[1].astype(F32), gain2_ref, t, n2_ref)
    for copy in (first, second, third):
        copy.wait_send()


def flipped(q, r):
    return (q // 2 + r // 2) % 2 * 2 + (q + r) % 2


def layer_kernel(
    peers,
    stream_hbm,
    conv_hbm,
    state_hbm,
    gain_hbm,
    branch_hbm,
    gate_hbm,
    taps_hbm,
    rmap_hbm,
    imap_hbm,
    decay_hbm,
    out_hbm,
    gain2_hbm,
    ids_hbm,
    weights_hbm,
    scale_hbm,
    eg_hbm,
    eu_hbm,
    ed_hbm,
    dg_hbm,
    du_hbm,
    dd_hbm,
    result_hbm,
    new_state_hbm,
    new_conv_hbm,
    stream_ref,
    conv_ref,
    state_ref,
    gain_ref,
    branch_w,
    gate_w,
    taps_ref,
    rmap_ref,
    imap_ref,
    decay_ref,
    out_w,
    gain2_ref,
    ids_ref,
    weights_ref,
    scale_ref,
    eg,
    eu,
    ed,
    dg,
    du,
    dd,
    result_ref,
    new_state_ref,
    new_conv_ref,
    eg_peer,
    eu_peer,
    ed_peer,
    peer_ref,
    nrm_ref,
    mix_ref,
    res_ref,
    dhid,
    inc,
    snd,
    got_d,
    got_dz,
    got_x,
    got_y,
    zbuf,
    got_z,
    fin_x,
    fin_y,
    fin_o,
    base_ref,
    wsend,
    wrecv,
    load_sem,
    store_sem,
    m_send,
    m_recv,
    mix_send,
    mix_recv,
    e_send,
    e_recv,
    w_send,
    w_recv,
    link_send,
    link_recv,
    back_send,
    back_recv,
    fin_send,
    fin_recv,
    dz_send,
    dz_recv,
):
    e = lax.axis_index("ep")
    t = lax.axis_index("tp")
    partner = {"tp": 1 - t}
    depth = peers // 4
    z = e // 4
    q = e % 4
    x_near = 4 * z + flipped(q, 1)
    y_near = 4 * z + flipped(q, 2)
    rows, width = stream_ref.shape
    half = rows // 2
    mine = pl.ds(pl.multiple_of(half * t, half), half)
    pairs = (
        (stream_hbm, stream_ref),
        (gain_hbm, gain_ref),
        (branch_hbm, branch_w),
        (gate_hbm, gate_w),
        (conv_hbm, conv_ref),
        (taps_hbm, taps_ref),
        (rmap_hbm, rmap_ref),
        (imap_hbm, imap_ref),
        (decay_hbm, decay_ref),
        (state_hbm, state_ref),
        (out_hbm, out_w),
        (gain2_hbm, gain2_ref),
        (ids_hbm, ids_ref),
        (weights_hbm, weights_ref),
        (scale_hbm, scale_ref),
        (dg_hbm, dg),
        (du_hbm, du),
        (dd_hbm, dd),
        (eg_hbm, eg),
        (eu_hbm, eu),
        (ed_hbm, ed),
    )
    loads = [pltpu.make_async_copy(a, b, load_sem.at[i]) for i, (a, b) in enumerate(pairs)]
    for i in (0, 1, 12, 13, 2, 3, 4, 5, 6, 7, 8, 9):
        loads[i].start()
    barrier = pltpu.get_barrier_semaphore()
    pl.semaphore_signal(barrier, inc=1, device_id=partner, device_id_type=pl.DeviceIdType.MESH)

    @pl.loop(1, peers)
    def _(offset):
        for core in range(2):
            pl.semaphore_signal(
                barrier,
                inc=1,
                device_id={"ep": lax.rem(e + offset, peers), "tp": core},
                device_id_type=pl.DeviceIdType.MESH,
            )

    loads[0].wait()
    pl.semaphore_wait(barrier, 2 * peers - 1)
    first = remote(stream_ref, peer_ref, m_send.at[0], m_recv.at[0], partner)
    first.start()
    own = stream_ref[...].astype(F32)
    own_sums = row_sums(own)

    loads[12].wait()
    loads[13].wait()
    ids = ids_ref[...]
    weights = weights_ref[...]
    lanes = wsend.shape[2]
    for d in range(peers):
        row = jnp.sum(jnp.where(ids == d, weights, 0.0), axis=0, keepdims=True)
        wsend[d] = jnp.concatenate([row, jnp.zeros((1, lanes - rows), F32)], axis=1)

    def weighing(r, o):
        there = (z + o) % depth
        d = 4 * there + flipped(q, r)
        slot = 4 * z + r
        return remote(wsend.at[d], wrecv.at[slot], w_send.at[d], w_recv.at[slot], {"ep": d})

    places = [(r, o) for r in range(4) for o in range(depth) if r or o]
    for r, o in places:
        weighing(r, o).start()

    loads[1].wait()
    first.wait_recv()
    norm_pair(own, own_sums, peer_ref[...].astype(F32), gain_ref, t, nrm_ref)
    for load in loads[2:10]:
        load.wait()
    for i in (10, 11, 14, 15, 16, 17, 18, 19, 20):
        loads[i].start()
    pushes = [
        remote(a, b, e_send.at[i], e_recv.at[i], partner)
        for i, (a, b) in enumerate(((eg_hbm, eg_peer), (eu_hbm, eu_peer), (ed_hbm, ed_peer)))
    ]
    pushes[0].start()
    block = rmap_ref.shape[1]
    chunk = 2 * block
    for c in range(width // chunk):
        cols = pl.ds(c * chunk, chunk)
        branch = dot(nrm_ref[0], branch_w[t, :, cols]) + dot(nrm_ref[1], branch_w[1 - t, :, cols])
        branch = branch.astype(BF16)
        gate = dot(nrm_ref[0], gate_w[t, :, cols]) + dot(nrm_ref[1], gate_w[1 - t, :, cols])
        gate = gate.astype(BF16).astype(F32)
        conv = branch.astype(F32) * taps_ref[3:4, cols]
        for i in range(3):
            conv = conv + conv_ref[i, :, cols].astype(F32) * taps_ref[i : i + 1, cols]
        conv = conv.astype(BF16)
        new_conv_ref[0, :, cols] = conv_ref[1, :, cols]
        new_conv_ref[1, :, cols] = conv_ref[2, :, cols]
        new_conv_ref[2, :, cols] = branch
        rec, inp = [], []
        for b in range(2):
            piece = conv[:, b * block : (b + 1) * block]
            rec.append(dot(piece, rmap_ref[2 * c + b]))
            inp.append(dot(piece, imap_ref[2 * c + b]))
        recur_gate = jax.nn.sigmoid(jnp.concatenate(rec, axis=1))
        input_gate = jax.nn.sigmoid(jnp.concatenate(inp, axis=1))
        logit = -decay_ref[:, cols]
        softplus = jnp.maximum(logit, 0.0) + jnp.log1p(jnp.exp(-jnp.abs(logit)))
        log_decay = -8.0 * recur_gate * softplus
        driven = jnp.sqrt(neg_expm1(2.0 * log_decay)) * (input_gate * conv.astype(F32))
        state = jnp.exp(log_decay) * state_ref[:, cols] + driven
        new_state_ref[:, cols] = state
        gelu = 0.5 * gate * (1.0 + jnp.tanh(0.7978845608028654 * (gate + 0.044715 * gate**3)))
        mix_ref[0, :, cols] = (gelu * state).astype(BF16)
    second = remote(mix_ref.at[0], mix_ref.at[1], mix_send.at[0], mix_recv.at[0], partner)
    second.start()
    stores = [
        pltpu.make_async_copy(new_state_ref, new_state_hbm, store_sem.at[0]),
        pltpu.make_async_copy(new_conv_ref, new_conv_hbm, store_sem.at[1]),
    ]
    for store in stores:
        store.start()
    loads[10].wait()
    base_ref[...] = dot(mix_ref[0], out_w[t])
    second.wait_recv()
    mixed = (base_ref[...] + dot(mix_ref[1], out_w[1 - t])).astype(BF16)
    resid = (own + mixed.astype(F32)).astype(BF16)
    res_ref[0] = resid
    third = remote(res_ref.at[0], res_ref.at[1], m_send.at[1], m_recv.at[1], partner)
    third.start()
    resid = resid.astype(F32)
    sums = row_sums(resid)
    loads[11].wait()
    third.wait_recv()
    norm_pair(resid, sums, res_ref[1].astype(F32), gain2_ref, t, nrm_ref)
    inc[4 * z, t] = nrm_ref[0, mine, :]
    inc[4 * z, 1 - t] = nrm_ref[1, mine, :]

    turn = 1 + z // 2 * 2
    mid = (z % 3 + 1) // 2
    o_b = 2 + mid
    o_c = 3 - mid

    def at(o):
        return (z + o * turn) % depth

    def z_copy(o, h):
        here = inc.at[4 * z, h]
        there = {"ep": 4 * at(o) + q}
        return remote(here, here, link_send.at[0, o, h], link_recv.at[0, z, h], there)

    def z_relay(o, h):
        j = at(o)
        here = inc.at[4 * j, h]
        there = {"ep": 4 * at(4 - o) + q}
        return remote(here, here, dz_send.at[2, o - 1, h], link_recv.at[0, j, h], there)

    def z_wait(o, h):
        j = at(o)
        here = inc.at[4 * j, h]
        remote(here, here, link_send.at[0, j, h], link_recv.at[0, j, h], partner).wait_recv()

    def side_copy(r, o, h):
        j = at(o)
        return remote(
            inc.at[4 * j, h],
            inc.at[4 * j + r, h],
            link_send.at[r, j, h],
            link_recv.at[r, j, h],
            {"ep": x_near if r == 1 else y_near},
        )

    def d_copy(h, o):
        j = at(o)
        return remote(
            inc.at[4 * j + 1 + h, h],
            inc.at[4 * j + 3, h],
            link_send.at[3, j, h],
            link_recv.at[3, j, h],
            {"ep": x_near if h else y_near},
        )

    def sides(o):
        side_copy(1, o, 0).start()
        side_copy(2, o, 1).start()
        side_copy(1, o, 1).start()
        side_copy(2, o, 0).start()

    def z_in(o, h):
        z_wait(o, h)
        z_relay(o, h).start()

    def along(o):
        z_wait(o, 0)
        side_copy(1, o, 0).start()
        z_wait(o, 1)
        side_copy(2, o, 1).start()
        side_copy(1, o, 1).start()
        side_copy(2, o, 0).start()

    def along_both():
        z_in(1, 0)
        side_copy(1, 1, 0).start()
        z_in(3, 0)
        side_copy(1, 3, 0).start()
        for o in (1, 3):
            z_in(o, 1)
            side_copy(2, o, 1).start()
            side_copy(1, o, 1).start()
            side_copy(2, o, 0).start()

    def dz_copy(o, h):
        here = inc.at[4 * z + 3, h]
        there = {"ep": 4 * at(o) + q}
        return remote(here, here, dz_send.at[0, o, h], link_recv.at[3, z, h], there)

    def dz_relay(o, h):
        j = at(o)
        here = inc.at[4 * j + 3, h]
        there = {"ep": 4 * at(4 - o) + q}
        return remote(here, here, dz_send.at[1, o, h], link_recv.at[3, j, h], there)

    def dz():
        for h in range(2):
            d_copy(h, 0).wait_recv()
            dz_copy(1, h).start()

            @pl.when(mid == 1)
            def _():
                dz_copy(3, h).start()

    def dzr():
        @pl.when(mid == 1)
        def _():
            for h in range(2):
                d_copy(h, 1).wait_recv()
                dz_relay(1, h).start()

    def near(o):
        for h in range(2):
            side_copy(1 + h, o, h).wait_recv()
            d_copy(h, o).start()

    def near_sides(o):
        side_copy(1, o, 0).wait_recv()
        side_copy(2, o, 1).wait_recv()

    spread = lax.broadcasted_iota(jnp.int32, (half, lanes), 0) + half * t == (
        lax.broadcasted_iota(jnp.int32, (half, lanes), 1)
    )

    def arrived_sides(o):
        side_copy(1, o, 1).wait_recv()
        side_copy(2, o, 0).wait_recv()

    def arrived(o):
        arrived_sides(o)
        if not (isinstance(o, int) and o == 0):
            for h in range(2):
                d_copy(h, o).wait_recv()

    def arr_end(o):
        arrived_sides(o)

        @pl.when(mid == 0)
        def _():
            for h in range(2):
                d_copy(h, o).wait_recv()

    def serve(o):
        slot = 4 * at(o)
        part = pl.ds(slot, 4)
        cols = []
        for r in range(4):
            cols.append(jnp.sum(jnp.where(spread, wrecv[slot + r], 0.0), axis=1, keepdims=True))
        scale = jnp.concatenate(cols, axis=0)
        low = inc[part, 0].reshape(4 * half, width)
        high = inc[part, 1].reshape(4 * half, width)
        hidden = []
        for gate_e, up_e in ((eg, eu), (eg_peer, eu_peer)):
            gate = dot(low, gate_e[0]) + dot(high, gate_e[1])
            up = dot(low, up_e[0]) + dot(high, up_e[1])
            hidden.append((jax.nn.silu(gate) * up).astype(BF16))
        for h, down in ((t, ed), (1 - t, ed_peer)):
            served = (dot(hidden[0], down[t]) + dot(hidden[1], down[1 - t])) * scale
            snd[part, h] = served.astype(BF16).reshape(4, half, width)

    def d_back(h, o):
        j = at(o)
        return remote(
            snd.at[4 * j + 3, h],
            got_d.at[j, h],
            back_send.at[3, j, h],
            back_recv.at[3, j, h],
            {"ep": x_near if h else y_near},
        )

    def side_back(r, o, h):
        j = at(o)
        near_chip = x_near if r == 1 else y_near
        if isinstance(o, int) and o == 0:
            return remote(
                snd.at[4 * j + r, h],
                (fin_x if r == 1 else fin_y).at[mine],
                back_send.at[r, j, h],
                fin_recv.at[r, t],
                {"ep": near_chip, "tp": h},
            )
        return remote(
            snd.at[4 * j + r, h],
            (got_x if r == 1 else got_y).at[j, h],
            back_send.at[r, j, h],
            back_recv.at[r, j, h],
            {"ep": near_chip},
        )

    def dz_back(o, h):
        j = at(o)
        there = {"ep": 4 * j + q}
        return remote(
            snd.at[4 * j + 3, h], got_dz.at[z, h], dz_send.at[3, o, h], dz_recv.at[z, h], there
        )

    def merge(slot, h, *parts):
        total = snd[slot, h].astype(F32)
        for part in parts:
            total = total + part.astype(F32)
        snd[slot, h] = total.astype(BF16)

    def send_all(o):
        for h in range(2):
            side_back(1, o, h).start()
            side_back(2, o, 1 - h).start()

    def send_first(o):
        d_back(0, o).start()
        d_back(1, o).start()
        side_back(1, o, 1).start()
        side_back(2, o, 0).start()

    def joined(o):
        j = at(o)
        for h in range(2):
            d_back(h, o).wait_recv()
            merge(4 * j + 1 + h, h, got_d[j, h])
            side_back(1 + h, o, h).start()

    def dz_wait(o, h):
        j = at(o)
        here = got_dz.at[j, h]
        remote(here, here, dz_send.at[3, o, h], dz_recv.at[j, h], partner).wait_recv()

    def send_own():
        @pl.when(mid == 1)
        def _():
            for h in range(2):
                dz_wait(3, h)
                dz_wait(2, h)
                merge(4 * z + 3, h, got_dz[at(3), h], got_dz[at(2), h])

        for h in range(2):
            dz_wait(1, h)
            merge(4 * z + 3, h, got_dz[at(1), h])
            d_back(h, 0).start()

    def bz_copy(o, h):
        j = at(o)
        return remote(
            zbuf.at[j, h],
            got_z.at[z, mine],
            back_send.at[0, j, h],
            back_recv.at[0, z, t],
            {"ep": 4 * j + q, "tp": h},
        )

    def bz_wait(o, core):
        j = at(o)
        here = got_z.at[j, pl.ds(core * half, half)]
        remote(here, here, back_send.at[0, j, 0], back_recv.at[0, j, core], partner).wait_recv()

    def home(o):
        j = at(o)
        for h in range(2):
            side_back(1, o, h).wait_recv()
            side_back(2, o, h).wait_recv()
            total = snd[4 * j, h].astype(F32) + got_x[j, h].astype(F32) + got_y[j, h].astype(F32)
            zbuf[j, h] = total.astype(BF16)
            bz_copy(o, h).start()

    own_copy = remote(snd.at[4 * z, 1 - t], fin_o, fin_send.at[0], fin_recv.at[0, 0], partner)

    for o in (1, 3):
        for h in range(2):
            z_copy(o, h).start()
    sides(0)
    pushes[1].start()
    pushes[2].start()

    for load in loads[14:18]:
        load.wait()
    dense_gate = dot(nrm_ref[0], dg[t]) + dot(nrm_ref[1], dg[1 - t])
    dense_up = dot(nrm_ref[0], du[t]) + dot(nrm_ref[1], du[1 - t])
    dhid[0] = (jax.nn.silu(dense_gate) * dense_up).astype(BF16)
    dense_copy = remote(dhid.at[0], dhid.at[1], m_send.at[2], m_recv.at[2], partner)
    dense_copy.start()
    near(0)

    @pl.when(mid == 1)
    def _():
        along_both()

    @pl.when(mid == 0)
    def _():
        along(1)

    for r, o in places:
        slot = 4 * ((z + o) % depth) + r
        remote(wsend.at[0], wrecv.at[slot], w_send.at[0], w_recv.at[slot], partner).wait_recv()
    row = jnp.sum(jnp.where(ids == e, weights, 0.0), axis=0, keepdims=True)
    wrecv[4 * z] = jnp.concatenate([row, jnp.zeros((1, lanes - rows), F32)], axis=1)
    dense = dot(dhid[0], dd[t])
    dense_copy.wait_recv()
    dense = (dense + dot(dhid[1], dd[1 - t])).astype(BF16)
    base_ref[...] = resid + scale_ref[...] * dense.astype(F32)
    for load in loads[18:]:
        load.wait()
    for push in pushes:
        push.wait_recv()

    @pl.when(mid == 0)
    def _():
        along(3)

    dz()
    along(2)
    arrived(0)
    serve(0)
    own_copy.start()
    dzr()
    near(o_c)
    near_sides(1)
    arr_end(1)
    serve(1)

    @pl.when(mid == 1)
    def _():
        dz_back(1, 0).start()
        dz_back(1, 1).start()


    @pl.when(mid == 0)
    def _():
        dz_back(1, 0).start()
        dz_back(1, 1).start()

    send_all(1)

    @pl.when(mid == 1)
    def _():
        near_sides(3)

    arrived(3)
    serve(3)

    @pl.when(mid == 1)
    def _():
        dz_back(3, 0).start()
        dz_back(3, 1).start()
        side_back(1, 3, 0).start()
        side_back(2, 3, 1).start()


    @pl.when(mid == 0)
    def _():
        send_first(3)


    @pl.when(mid == 0)
    def _():
        near_sides(2)

    arrived(2)
    serve(2)

    @pl.when(mid == 0)
    def _():
        dz_back(2, 0).start()
        dz_back(2, 1).start()
        side_back(1, 2, 0).start()
        side_back(2, 2, 1).start()


    @pl.when(mid == 1)
    def _():
        send_first(2)
        side_back(1, 3, 1).start()
        side_back(2, 3, 0).start()

    home(1)
    joined(o_c)

    @pl.when(mid == 0)
    def _():
        side_back(1, 2, 1).start()
        side_back(2, 2, 0).start()

    side_back(1, 0, 1).start()
    side_back(2, 0, 0).start()
    send_own()
    home(o_c)
    home(o_b)
    joined(0)
    other = pl.ds(pl.multiple_of(half - half * t, half), half)
    base_ref[mine, :] += snd[4 * z, t].astype(F32)
    own_copy.wait_recv()
    base_ref[other, :] += fin_o[...].astype(F32)
    total = base_ref[...]
    for o in (1, 3, 2):
        for core in range(2):
            bz_wait(o, core)
        total = total + got_z[at(o)].astype(F32)
    for r, fin in ((1, fin_x), (2, fin_y)):
        for core in range(2):
            here = fin.at[pl.ds(core * half, half)]
            remote(here, here, fin_send.at[1], fin_recv.at[r, core], partner).wait_recv()
        total = total + fin[...].astype(F32)
    result_ref[...] = total.astype(BF16)
    stores.append(pltpu.make_async_copy(result_ref, result_hbm, store_sem.at[2]))
    stores[-1].start()
    for copy in (first, third, dense_copy, own_copy, second, *pushes):
        copy.wait_send()
    for r, o in places:
        weighing(r, o).wait_send()
    for o in range(depth):
        for h in range(2):
            if o:
                bz_copy(o, h).wait_send()
            if o in (1, 3):
                z_copy(o, h).wait_send()
            for r in (1, 2):
                side_copy(r, o, h).wait_send()
                side_back(r, o, h).wait_send()
        if o == 0:
            for h in range(2):
                d_copy(h, o).wait_send()
                d_back(h, o).wait_send()

    @pl.when(mid == 1)
    def _():
        for h in range(2):
            z_relay(1, h).wait_send()
            z_relay(3, h).wait_send()
            dz_relay(1, h).wait_send()
            dz_copy(3, h).wait_send()
            dz_back(3, h).wait_send()

    @pl.when(mid == 0)
    def _():
        for h in range(2):
            dz_back(2, h).wait_send()

    for h in range(2):
        d_copy(h, o_c).wait_send()
        d_back(h, o_c).wait_send()
        dz_copy(1, h).wait_send()
        dz_back(1, h).wait_send()

    for store in stores:
        store.wait()


def expert_kernel(
    full,
    peers,
    group,
    n2_ref,
    out_ref,
    resid_ref,
    ids_ref,
    weights_ref,
    scale_ref,
    eg_hbm,
    eu_hbm,
    ed_hbm,
    dg_hbm,
    du_hbm,
    dd_hbm,
    *refs,
):
    if full:
        result_ref, *refs = refs
    else:
        dense_ref, back_ref, *refs = refs
    (
        eg,
        eu,
        ed,
        dg,
        du,
        dd,
        inc,
        hid,
        src,
        ret,
        dhid,
        load_sem,
        own_sem,
        x_send,
        x_recv,
        f_send,
        f_recv,
        h_send,
        h_recv,
        r_send,
        r_recv,
        d_sem,
    ) = refs
    e = lax.axis_index("ep")
    t = lax.axis_index("tp")
    partner = {"tp": 1 - t}
    groups = peers // group
    cap = inc.shape[2]
    width = inc.shape[3]
    loads = [
        pltpu.make_async_copy(a, b, load_sem.at[i])
        for i, (a, b) in enumerate(
            ((dg_hbm, dg), (du_hbm, du), (dd_hbm, dd), (eg_hbm, eg), (eu_hbm, eu), (ed_hbm, ed))
        )
    ]
    for load in loads:
        load.start()

    def outgoing(offset):
        return n2_ref.at[0] if full else out_ref.at[lax.rem(e + offset, peers)]

    keep = pltpu.make_async_copy(outgoing(0), inc.at[0, 0], own_sem)
    keep.start()
    barrier = pltpu.get_barrier_semaphore()
    pl.semaphore_signal(barrier, inc=1, device_id=partner, device_id_type=pl.DeviceIdType.MESH)

    @pl.loop(1, peers)
    def _(offset):
        pl.semaphore_signal(
            barrier,
            inc=1,
            device_id={"ep": lax.rem(e + offset, peers)},
            device_id_type=pl.DeviceIdType.MESH,
        )

    pl.semaphore_wait(barrier, peers)

    def sending(offset):
        return remote(
            outgoing(offset),
            inc.at[0, offset],
            x_send.at[offset],
            x_recv.at[offset],
            {"ep": lax.rem(e + offset, peers)},
        )

    @pl.loop(1, peers)
    def _(offset):
        sending(offset).start()

    for load in loads[:3]:
        load.wait()
    rows0, rows1 = n2_ref[0], n2_ref[1]
    dense_gate = dot(rows0, dg[t]) + dot(rows1, dg[1 - t])
    dense_up = dot(rows0, du[t]) + dot(rows1, du[1 - t])
    dhid[0] = (jax.nn.silu(dense_gate) * dense_up).astype(BF16)
    dense_copy = remote(dhid.at[0], dhid.at[1], d_sem.at[0], d_sem.at[1], partner)
    dense_copy.start()
    dense = dot(dhid[0], dd[t])
    dense_copy.wait()
    dense = (dense + dot(dhid[1], dd[1 - t])).astype(BF16)
    keep.wait()
    for load in loads[3:]:
        load.wait()

    def forwarding(g):
        part = pl.ds(g * group, group)
        return remote(inc.at[0, part], inc.at[1, part], f_send.at[g], f_recv.at[g], partner)

    def hiding(g):
        part = pl.ds(g * group, group)
        return remote(hid.at[0, part], hid.at[1, part], h_send.at[g], h_recv.at[g], partner)

    def returning(offset):
        return remote(
            src.at[offset],
            ret.at[offset],
            r_send.at[offset],
            r_recv.at[offset],
            {"ep": lax.rem(e + peers - offset, peers)},
        )

    def arrive(g):
        @pl.loop(max(1, g * group), (g + 1) * group)
        def _(offset):
            sending(offset).wait_recv()

        forwarding(g).start()

    def upward(g):
        forwarding(g).wait_recv()
        part = pl.ds(g * group, group)
        own = inc[0, part].reshape(group * cap, width)
        peer = inc[1, part].reshape(group * cap, width)
        gate = dot(own, eg[t]) + dot(peer, eg[1 - t])
        up = dot(own, eu[t]) + dot(peer, eu[1 - t])
        hidden = (jax.nn.silu(gate) * up).astype(BF16)
        hid[0, part] = hidden.reshape(group, cap, -1)
        hiding(g).start()

    def downward(g):
        hiding(g).wait_recv()
        part = pl.ds(g * group, group)
        own = hid[0, part].reshape(group * cap, -1)
        peer = hid[1, part].reshape(group * cap, -1)
        served = dot(own, ed[t]) + dot(peer, ed[1 - t])
        src[part] = served.astype(BF16).reshape(group, cap, width)

        @pl.loop(max(1, g * group), (g + 1) * group)
        def _(offset):
            returning(offset).start()

    for step in range(groups + 2):
        if step < groups:
            arrive(step)
        if 1 <= step <= groups:
            upward(step - 1)
        if step >= 2:
            downward(step - 2)

    if full:
        total = resid_ref[...].astype(F32) + scale_ref[...] * dense.astype(F32)
        ids = ids_ref[...]
        weights = weights_ref[...]

        def weight(offset):
            chosen = ids == lax.rem(e + offset, peers)
            return jnp.sum(jnp.where(chosen, weights, 0.0), axis=1, keepdims=True)

        routed = weight(0) * src[0].astype(F32)
        for offset in range(1, peers):
            returning(offset).wait_recv()
            routed = routed + weight(offset) * ret[offset].astype(F32)
        result_ref[...] = (total + routed).astype(BF16)
    else:
        dense_ref[...] = dense
        back_ref[0] = src[0]

        @pl.loop(1, peers)
        def _(offset):
            returning(offset).wait_recv()
            back_ref[offset] = ret[offset]

    @pl.loop(1, peers)
    def _(offset):
        sending(offset).wait_send()
        returning(offset).wait_send()

    @pl.loop(0, groups)
    def _(g):
        forwarding(g).wait_send()
        hiding(g).wait_send()


def emit_kernel(a_in, b_in, c_in, a_out, b_out, c_out, a, b, c, sem):
    sets = tuple(enumerate(((a_in, a, a_out), (b_in, b, b_out), (c_in, c, c_out))))
    reads = [pltpu.make_async_copy(src, mid, sem.at[0, i]) for i, (src, mid, _) in sets]
    writes = [pltpu.make_async_copy(mid, dst, sem.at[1, i]) for i, (_, mid, dst) in sets]
    for read in reads:
        read.start()
    for read, write in zip(reads, writes):
        read.wait()
        write.start()
    for write in writes:
        write.wait()


def halves(weight):
    return weight.reshape(2, weight.shape[0] // 2, weight.shape[1])


def per_device(
    stream,
    conv_state,
    recur_state,
    mix_gain,
    branch_weight,
    gate_weight,
    conv_taps,
    recur_map,
    input_map,
    decay_logit,
    out_weight,
    moe_gain,
    route_ids,
    route_weights,
    expert_gate,
    expert_up,
    expert_down,
    dense_gate,
    dense_up,
    dense_down,
    dense_scale,
):
    rows, width = stream.shape
    dma = pltpu.SemaphoreType.DMA
    top = route_ids.shape[1]
    peers = lax.axis_size("ep")
    cap = max(2, min(rows, 3 * rows * top // peers))
    if cap == rows and peers // 4 == 4:
        operands = (
            stream,
            conv_state.transpose(1, 0, 2),
            recur_state,
            mix_gain.reshape(2, 1, width),
            halves(branch_weight),
            halves(gate_weight),
            conv_taps,
            recur_map,
            input_map,
            decay_logit.reshape(1, width),
            halves(out_weight),
            moe_gain.reshape(2, 1, width),
            route_ids.T,
            route_weights.T,
            dense_scale.reshape(1, width),
            halves(expert_gate[0]),
            halves(expert_up[0]),
            halves(expert_down[0]),
            halves(dense_gate),
            halves(dense_up),
            halves(dense_down),
        )
        depth = peers // 4
        half = rows // 2
        lanes = -(-rows // 128) * 128
        outs = (
            jax.ShapeDtypeStruct((rows, width), BF16),
            jax.ShapeDtypeStruct((rows, width), F32),
            jax.ShapeDtypeStruct((3, rows, width), BF16),
        )
        column = pltpu.VMEM((depth, 2, half, width), BF16)
        whole = pltpu.VMEM((rows, width), BF16)
        result, new_state, new_conv = pl.pallas_call(
            functools.partial(layer_kernel, peers),
            out_shape=outs,
            in_specs=[ANY] * len(operands),
            out_specs=[ANY] * 3,
            scratch_shapes=[pltpu.VMEM(a.shape, a.dtype) for a in operands + outs + operands[15:18]]
            + [whole]
            + [pltpu.VMEM((2, rows, width), BF16)] * 3
            + [pltpu.VMEM((2, rows, dense_gate.shape[1]), BF16)]
            + [pltpu.VMEM((peers, 2, half, width), BF16)] * 2
            + [column] * 5
            + [pltpu.VMEM((depth, rows, width), BF16)]
            + [whole] * 2
            + [pltpu.VMEM((half, width), BF16), pltpu.VMEM((rows, width), F32)]
            + [pltpu.VMEM((peers, 1, lanes), F32)] * 2
            + [dma((len(operands),)), dma((3,))]
            + [dma((3,))] * 2
            + [dma((1,))] * 2
            + [dma((3,))] * 2
            + [dma((peers,))] * 2
            + [dma((4, depth, 2))] * 4
            + [dma((2,)), dma((3, 2)), dma((4, depth, 2)), dma((depth, 2))],
            compiler_params=pltpu.CompilerParams(
                collective_id=2, has_side_effects=True, vmem_limit_bytes=63 * 1024 * 1024
            ),
            name="layer",
        )(*operands)
        result, new_state, new_conv = pl.pallas_call(
            emit_kernel,
            out_shape=tuple(jax.ShapeDtypeStruct(a.shape, a.dtype) for a in (result, new_state, new_conv)),
            in_specs=[ANY] * 3,
            out_specs=[ANY] * 3,
            scratch_shapes=[pltpu.VMEM(a.shape, a.dtype) for a in (result, new_state, new_conv)]
            + [dma((2, 3))],
            compiler_params=pltpu.CompilerParams(vmem_limit_bytes=63 * 1024 * 1024),
            name="emit",
        )(result, new_state, new_conv)
        return result, new_state, new_conv.transpose(1, 0, 2)
    conv_part = sum(conv_state[:, i].astype(F32) * conv_taps[i] for i in range(3))
    branch_in, new_state, resid, n2 = pl.pallas_call(
        mixer_kernel,
        out_shape=(
            jax.ShapeDtypeStruct((rows, width), BF16),
            jax.ShapeDtypeStruct((rows, width), F32),
            jax.ShapeDtypeStruct((rows, width), BF16),
            jax.ShapeDtypeStruct((2, rows, width), BF16),
        ),
        in_specs=[VMEM] * 4 + [ANY] * 2 + [VMEM] * 4 + [ANY, VMEM],
        out_specs=[VMEM] * 4,
        scratch_shapes=[pltpu.VMEM((2, width, width), BF16)] * 3
        + [pltpu.VMEM((rows, width), BF16)]
        + [pltpu.VMEM((2, rows, width), BF16)] * 3
        + [dma((3,))] * 3,
        compiler_params=pltpu.CompilerParams(
            collective_id=0, has_side_effects=True, vmem_limit_bytes=48 * 1024 * 1024
        ),
        name="mixer",
    )(
        stream,
        conv_part,
        recur_state,
        mix_gain.reshape(2, 1, width),
        halves(branch_weight),
        halves(gate_weight),
        conv_taps,
        recur_map,
        input_map,
        decay_logit.reshape(1, width),
        halves(out_weight),
        moe_gain.reshape(2, 1, width),
    )
    new_conv = jnp.concatenate([conv_state[:, 1:], branch_in[:, None]], axis=1)

    full = cap == rows
    if full:
        outgoing = jnp.zeros((8, 128), BF16)
    else:
        cap = -(-cap // 16) * 16
        flat_ids = route_ids.reshape(-1)
        one_hot = (flat_ids[:, None] == jnp.arange(peers, dtype=jnp.int32)[None, :]).astype(jnp.int32)
        rank = jnp.sum(one_hot * (jnp.cumsum(one_hot, axis=0) - 1), axis=1)
        slots = (flat_ids * cap + rank).reshape(rows, top)
        table = jnp.sum(
            (slots[:, :, None] == jnp.arange(peers * cap, dtype=jnp.int32)).astype(BF16), axis=1
        )
        outgoing = lax.dot_general(
            table, n2[0], (((0,), (0,)), ((), ())), preferred_element_type=F32
        )
        outgoing = outgoing.astype(BF16).reshape(peers, cap, width)
    group = max(1, min(peers, 256 // cap))
    while peers % group:
        group -= 1
    groups = peers // group
    hidden = expert_gate.shape[2]
    out_shape = [jax.ShapeDtypeStruct((rows, width), BF16)]
    if not full:
        out_shape.append(jax.ShapeDtypeStruct((peers, cap, width), BF16))
    outs = pl.pallas_call(
        functools.partial(expert_kernel, full, peers, group),
        out_shape=out_shape,
        in_specs=[VMEM] * 6 + [ANY] * 6,
        out_specs=[VMEM] * len(out_shape),
        scratch_shapes=[
            pltpu.VMEM((2, width, hidden), BF16),
            pltpu.VMEM((2, width, hidden), BF16),
            pltpu.VMEM((2, hidden, width), BF16),
            pltpu.VMEM((2, width, dense_gate.shape[1]), BF16),
            pltpu.VMEM((2, width, dense_gate.shape[1]), BF16),
            pltpu.VMEM((2, dense_gate.shape[1], width), BF16),
            pltpu.VMEM((2, peers, cap, width), BF16),
            pltpu.VMEM((2, peers, cap, hidden), BF16),
            pltpu.VMEM((peers, cap, width), BF16),
            pltpu.VMEM((peers, cap, width), BF16),
            pltpu.VMEM((2, rows, dense_gate.shape[1]), BF16),
            dma((6,)),
            dma,
            dma((peers,)),
            dma((peers,)),
            dma((groups,)),
            dma((groups,)),
            dma((groups,)),
            dma((groups,)),
            dma((peers,)),
            dma((peers,)),
            dma((2,)),
        ],
        compiler_params=pltpu.CompilerParams(
            collective_id=1, has_side_effects=True, vmem_limit_bytes=56 * 1024 * 1024
        ),
        name="experts",
    )(
        n2,
        outgoing,
        resid,
        route_ids,
        route_weights,
        dense_scale.reshape(1, width),
        halves(expert_gate[0]),
        halves(expert_up[0]),
        halves(expert_down[0]),
        halves(dense_gate),
        halves(dense_up),
        halves(dense_down),
    )
    if full:
        return outs[0], new_state, new_conv
    dense_out, back = outs
    shifted = lax.rem(flat_ids - lax.axis_index("ep") + peers, peers)
    picked = back.reshape(peers * cap, width)[(shifted * cap + rank).reshape(rows, top)]
    routed = jnp.sum(picked.astype(F32) * route_weights[:, :, None], axis=1)
    result = (resid.astype(F32) + routed + dense_scale * dense_out.astype(F32)).astype(BF16)
    return result, new_state, new_conv


def solution(mesh):
    in_specs = (
        P("ep", "tp"),
        P("ep", None, "tp"),
        P("ep", "tp"),
        P(),
        P(None, "tp"),
        P(None, "tp"),
        P(None, "tp"),
        P("tp", None, None),
        P("tp", None, None),
        P("tp"),
        P(None, "tp"),
        P(),
        P("ep", None),
        P("ep", None),
        P("ep", None, "tp"),
        P("ep", None, "tp"),
        P("ep", None, "tp"),
        P(None, "tp"),
        P(None, "tp"),
        P(None, "tp"),
        P("tp"),
    )
    out_specs = (P("ep", "tp"), P("ep", "tp"), P("ep", None, "tp"))
    return jax.shard_map(
        per_device, mesh=mesh, in_specs=in_specs, out_specs=out_specs, check_vma=False
    )
```

```python
import functools

import jax
import jax.numpy as jnp
from jax import lax
from jax.experimental import pallas as pl
from jax.experimental.pallas import tpu as pltpu
from jax.sharding import PartitionSpec as P

BF16 = jnp.bfloat16
F32 = jnp.float32
VMEM = pl.BlockSpec(memory_space=pltpu.VMEM)
ANY = pl.BlockSpec(memory_space=pl.ANY)
HBM = pl.BlockSpec(memory_space=pltpu.HBM)


def dot(a, b):
    return jnp.dot(a, b, preferred_element_type=F32)


def remote(src, dst, send_sem, recv_sem, device):
    return pltpu.make_async_remote_copy(
        src_ref=src,
        dst_ref=dst,
        send_sem=send_sem,
        recv_sem=recv_sem,
        device_id=device,
        device_id_type=pl.DeviceIdType.MESH,
    )


def row_sums(rows):
    return (
        jnp.sum(rows, axis=1, keepdims=True),
        jnp.sum(rows * rows, axis=1, keepdims=True),
    )


def neg_expm1(y):
    series = 1.0 + y / 8.0
    for order in range(7, 1, -1):
        series = 1.0 + y / order * series
    return jnp.where(y > -0.3, -y * series, 1.0 - jnp.exp(y))


def norm_pair(own, own_sums, peer, gain_ref, t, out_ref):
    width = own.shape[1]
    peer_sums = row_sums(peer)
    mean = (own_sums[0] + peer_sums[0]) / (2 * width)
    var = (own_sums[1] + peer_sums[1]) / (2 * width) - mean * mean
    scale = lax.rsqrt(var + 1e-05)
    for slot, (rows, half) in enumerate(((own, t), (peer, 1 - t))):
        out_ref[slot] = ((rows - mean) * scale * gain_ref[half]).astype(BF16)


def mixer_kernel(
    stream_ref,
    part_ref,
    state_ref,
    gain_ref,
    branch_hbm,
    gate_hbm,
    taps_ref,
    rmap_ref,
    imap_ref,
    decay_ref,
    out_hbm,
    gain2_ref,
    branch_ref,
    new_state_ref,
    resid_ref,
    n2_ref,
    branch_w,
    gate_w,
    out_w,
    peer_ref,
    nrm_ref,
    mix_ref,
    res_ref,
    load_sem,
    send_sem,
    recv_sem,
):
    t = lax.axis_index("tp")
    partner = {"tp": 1 - t}
    loads = [
        pltpu.make_async_copy(src, dst, load_sem.at[i])
        for i, (src, dst) in enumerate(
            ((branch_hbm, branch_w), (gate_hbm, gate_w), (out_hbm, out_w))
        )
    ]
    for load in loads:
        load.start()
    barrier = pltpu.get_barrier_semaphore()
    pl.semaphore_signal(barrier, inc=1, device_id=partner, device_id_type=pl.DeviceIdType.MESH)
    pl.semaphore_wait(barrier, 1)
    first = remote(stream_ref, peer_ref, send_sem.at[0], recv_sem.at[0], partner)
    first.start()
    own = stream_ref[...].astype(F32)
    own_sums = row_sums(own)
    first.wait_recv()
    norm_pair(own, own_sums, peer_ref[...].astype(F32), gain_ref, t, nrm_ref)

    width = stream_ref.shape[1]
    block = rmap_ref.shape[1]
    chunk = 2 * block
    loads[0].wait()
    loads[1].wait()
    for c in range(width // chunk):
        cols = pl.ds(c * chunk, chunk)
        branch = dot(nrm_ref[0], branch_w[t, :, cols]) + dot(nrm_ref[1], branch_w[1 - t, :, cols])
        branch = branch.astype(BF16)
        branch_ref[:, cols] = branch
        gate = dot(nrm_ref[0], gate_w[t, :, cols]) + dot(nrm_ref[1], gate_w[1 - t, :, cols])
        gate = gate.astype(BF16).astype(F32)
        conv = (branch.astype(F32) * taps_ref[3:4, cols] + part_ref[:, cols]).astype(BF16)
        rec, inp = [], []
        for b in range(2):
            piece = conv[:, b * block : (b + 1) * block]
            rec.append(dot(piece, rmap_ref[2 * c + b]))
            inp.append(dot(piece, imap_ref[2 * c + b]))
        recur_gate = jax.nn.sigmoid(jnp.concatenate(rec, axis=1))
        input_gate = jax.nn.sigmoid(jnp.concatenate(inp, axis=1))
        logit = -decay_ref[:, cols]
        softplus = jnp.maximum(logit, 0.0) + jnp.log1p(jnp.exp(-jnp.abs(logit)))
        log_decay = -8.0 * recur_gate * softplus
        driven = jnp.sqrt(neg_expm1(2.0 * log_decay)) * (input_gate * conv.astype(F32))
        state = jnp.exp(log_decay) * state_ref[:, cols] + driven
        new_state_ref[:, cols] = state
        gelu = 0.5 * gate * (1.0 + jnp.tanh(0.7978845608028654 * (gate + 0.044715 * gate**3)))
        mix_ref[0, :, cols] = (gelu * state).astype(BF16)
    second = remote(mix_ref.at[0], mix_ref.at[1], send_sem.at[1], recv_sem.at[1], partner)
    second.start()
    loads[2].wait()
    mixed = dot(mix_ref[0], out_w[t])
    second.wait_recv()
    mixed = (mixed + dot(mix_ref[1], out_w[1 - t])).astype(BF16)
    resid = (own + mixed.astype(F32)).astype(BF16)
    res_ref[0] = resid
    third = remote(res_ref.at[0], res_ref.at[1], send_sem.at[2], recv_sem.at[2], partner)
    third.start()
    resid_ref[...] = resid
    resid = resid.astype(F32)
    sums = row_sums(resid)
    third.wait_recv()
    norm_pair(resid, sums, res_ref[1].astype(F32), gain2_ref, t, n2_ref)
    for copy in (first, second, third):
        copy.wait_send()


def flipped(q, r):
    return (q // 2 + r // 2) % 2 * 2 + (q + r) % 2


def layer_kernel(
    peers,
    stream_hbm,
    conv_hbm,
    state_hbm,
    gain_hbm,
    branch_hbm,
    gate_hbm,
    taps_hbm,
    rmap_hbm,
    imap_hbm,
    decay_hbm,
    out_hbm,
    gain2_hbm,
    ids_hbm,
    weights_hbm,
    scale_hbm,
    eg_hbm,
    eu_hbm,
    ed_hbm,
    dg_hbm,
    du_hbm,
    dd_hbm,
    result_hbm,
    new_state_hbm,
    new_conv_hbm,
    stream_ref,
    conv_ref,
    state_ref,
    gain_ref,
    branch_w,
    gate_w,
    taps_ref,
    rmap_ref,
    imap_ref,
    decay_ref,
    out_w,
    gain2_ref,
    ids_ref,
    weights_ref,
    scale_ref,
    eg,
    eu,
    ed,
    dg,
    du,
    dd,
    result_ref,
    new_state_ref,
    new_conv_ref,
    eg_peer,
    eu_peer,
    ed_peer,
    peer_ref,
    nrm_ref,
    mix_ref,
    res_ref,
    dhid,
    inc,
    snd,
    got_d,
    got_dz,
    got_x,
    got_y,
    zbuf,
    got_z,
    fin_x,
    fin_y,
    fin_o,
    base_ref,
    wsend,
    wrecv,
    load_sem,
    store_sem,
    m_send,
    m_recv,
    mix_send,
    mix_recv,
    e_send,
    e_recv,
    w_send,
    w_recv,
    link_send,
    link_recv,
    back_send,
    back_recv,
    fin_send,
    fin_recv,
    dz_send,
    dz_recv,
    res_send,
    res_recv,
):
    e = lax.axis_index("ep")
    t = lax.axis_index("tp")
    partner = {"tp": 1 - t}
    depth = peers // 4
    z = e // 4
    q = e % 4
    x_near = 4 * z + flipped(q, 1)
    y_near = 4 * z + flipped(q, 2)
    rows, width = stream_ref.shape
    half = rows // 2
    mine = pl.ds(pl.multiple_of(half * t, half), half)
    pairs = (
        (stream_hbm, stream_ref),
        (gain_hbm, gain_ref),
        (branch_hbm, branch_w),
        (gate_hbm, gate_w),
        (conv_hbm, conv_ref),
        (taps_hbm, taps_ref),
        (rmap_hbm, rmap_ref),
        (imap_hbm, imap_ref),
        (decay_hbm, decay_ref),
        (state_hbm, state_ref),
        (out_hbm, out_w),
        (gain2_hbm, gain2_ref),
        (ids_hbm, ids_ref),
        (weights_hbm, weights_ref),
        (scale_hbm, scale_ref),
        (dg_hbm, dg),
        (du_hbm, du),
        (dd_hbm, dd),
        (eg_hbm, eg),
        (eu_hbm, eu),
        (ed_hbm, ed),
    )
    loads = [pltpu.make_async_copy(a, b, load_sem.at[i]) for i, (a, b) in enumerate(pairs)]
    for i in (0, 1, 12, 13, 2, 3, 4, 5, 6, 7, 8, 9):
        loads[i].start()
    barrier = pltpu.get_barrier_semaphore()
    pl.semaphore_signal(barrier, inc=1, device_id=partner, device_id_type=pl.DeviceIdType.MESH)

    @pl.loop(1, peers)
    def _(offset):
        for core in range(2):
            pl.semaphore_signal(
                barrier,
                inc=1,
                device_id={"ep": lax.rem(e + offset, peers), "tp": core},
                device_id_type=pl.DeviceIdType.MESH,
            )

    loads[0].wait()
    pl.semaphore_wait(barrier, 2 * peers - 1)
    first = remote(stream_ref, peer_ref, m_send.at[0], m_recv.at[0], partner)
    first.start()
    own = stream_ref[...].astype(F32)
    own_sums = row_sums(own)

    loads[12].wait()
    loads[13].wait()
    ids = ids_ref[...]
    weights = weights_ref[...]
    lanes = wsend.shape[2]
    for d in range(peers):
        row = jnp.sum(jnp.where(ids == d, weights, 0.0), axis=0, keepdims=True)
        wsend[d] = jnp.concatenate([row, jnp.zeros((1, lanes - rows), F32)], axis=1)

    def weighing(r, o):
        there = (z + o) % depth
        d = 4 * there + flipped(q, r)
        slot = 4 * z + r
        return remote(wsend.at[d], wrecv.at[slot], w_send.at[d], w_recv.at[slot], {"ep": d})

    places = [(r, o) for r in range(4) for o in range(depth) if r or o]
    for r, o in places:
        weighing(r, o).start()

    loads[1].wait()
    first.wait_recv()
    norm_pair(own, own_sums, peer_ref[...].astype(F32), gain_ref, t, nrm_ref)
    for load in loads[2:10]:
        load.wait()
    for i in (10, 11, 14, 15, 16, 17, 18, 19, 20):
        loads[i].start()
    pushes = [
        remote(a, b, e_send.at[i], e_recv.at[i], partner)
        for i, (a, b) in enumerate(((eg_hbm, eg_peer), (eu_hbm, eu_peer), (ed_hbm, ed_peer)))
    ]
    pushes[0].start()
    block = rmap_ref.shape[1]
    chunk = 2 * block
    for c in range(width // chunk):
        cols = pl.ds(c * chunk, chunk)
        branch = dot(nrm_ref[0], branch_w[t, :, cols]) + dot(nrm_ref[1], branch_w[1 - t, :, cols])
        branch = branch.astype(BF16)
        gate = dot(nrm_ref[0], gate_w[t, :, cols]) + dot(nrm_ref[1], gate_w[1 - t, :, cols])
        gate = gate.astype(BF16).astype(F32)
        conv = branch.astype(F32) * taps_ref[3:4, cols]
        for i in range(3):
            conv = conv + conv_ref[i, :, cols].astype(F32) * taps_ref[i : i + 1, cols]
        conv = conv.astype(BF16)
        new_conv_ref[0, :, cols] = conv_ref[1, :, cols]
        new_conv_ref[1, :, cols] = conv_ref[2, :, cols]
        new_conv_ref[2, :, cols] = branch
        rec, inp = [], []
        for b in range(2):
            piece = conv[:, b * block : (b + 1) * block]
            rec.append(dot(piece, rmap_ref[2 * c + b]))
            inp.append(dot(piece, imap_ref[2 * c + b]))
        recur_gate = jax.nn.sigmoid(jnp.concatenate(rec, axis=1))
        input_gate = jax.nn.sigmoid(jnp.concatenate(inp, axis=1))
        logit = -decay_ref[:, cols]
        softplus = jnp.maximum(logit, 0.0) + jnp.log1p(jnp.exp(-jnp.abs(logit)))
        log_decay = -8.0 * recur_gate * softplus
        driven = jnp.sqrt(neg_expm1(2.0 * log_decay)) * (input_gate * conv.astype(F32))
        state = jnp.exp(log_decay) * state_ref[:, cols] + driven
        new_state_ref[:, cols] = state
        gelu = 0.5 * gate * (1.0 + jnp.tanh(0.7978845608028654 * (gate + 0.044715 * gate**3)))
        mix_ref[0, :, cols] = (gelu * state).astype(BF16)
    second = remote(mix_ref.at[0], mix_ref.at[1], mix_send.at[0], mix_recv.at[0], partner)
    second.start()
    stores = [
        pltpu.make_async_copy(new_state_ref, new_state_hbm, store_sem.at[0]),
        pltpu.make_async_copy(new_conv_ref, new_conv_hbm, store_sem.at[1]),
    ]
    for store in stores:
        store.start()
    loads[10].wait()
    base_ref[...] = dot(mix_ref[0], out_w[t])
    second.wait_recv()
    mixed = (base_ref[...] + dot(mix_ref[1], out_w[1 - t])).astype(BF16)
    resid = (own + mixed.astype(F32)).astype(BF16)
    res_ref[0] = resid
    other = pl.ds(pl.multiple_of(half - half * t, half), half)

    def res_copy(part, i):
        here, there = res_ref.at[0, part], res_ref.at[1, part]
        return remote(here, there, res_send.at[i], res_recv.at[i], partner)

    res_copy(other, 0).start()
    res_copy(mine, 1).start()
    resid = resid.astype(F32)
    loads[11].wait()
    base_ref[...] = resid
    res_copy(mine, 0).wait_recv()

    def norm_part(part):
        rows_f = base_ref[part, :]
        peer_f = res_ref[1, part, :].astype(F32)
        norm_pair(rows_f, row_sums(rows_f), peer_f, gain2_ref, t, nrm_ref.at[:, part, :])

    norm_part(mine)
    inc[4 * z, t] = nrm_ref[0, mine, :]
    inc[4 * z, 1 - t] = nrm_ref[1, mine, :]

    turn = 1 + z // 2 * 2
    mid = (z % 3 + 1) // 2
    o_b = 2 + mid
    o_c = 3 - mid

    def at(o):
        return (z + o * turn) % depth

    def z_copy(o, h):
        here = inc.at[4 * z, h]
        there = {"ep": 4 * at(o) + q}
        return remote(here, here, link_send.at[0, o, h], link_recv.at[0, z, h], there)

    def z_relay(o, h):
        j = at(o)
        here = inc.at[4 * j, h]
        there = {"ep": 4 * at(4 - o) + q}
        return remote(here, here, dz_send.at[2, o - 1, h], link_recv.at[0, j, h], there)

    def z_wait(o, h):
        j = at(o)
        here = inc.at[4 * j, h]
        remote(here, here, link_send.at[0, j, h], link_recv.at[0, j, h], partner).wait_recv()

    def side_copy(r, o, h):
        j = at(o)
        return remote(
            inc.at[4 * j, h],
            inc.at[4 * j + r, h],
            link_send.at[r, j, h],
            link_recv.at[r, j, h],
            {"ep": x_near if r == 1 else y_near},
        )

    def d_copy(h, o):
        j = at(o)
        return remote(
            inc.at[4 * j + 1 + h, h],
            inc.at[4 * j + 3, h],
            link_send.at[3, j, h],
            link_recv.at[3, j, h],
            {"ep": x_near if h else y_near},
        )

    def sides(o):
        side_copy(1, o, 0).start()
        side_copy(2, o, 1).start()
        side_copy(1, o, 1).start()
        side_copy(2, o, 0).start()

    def z_in(o, h):
        z_wait(o, h)
        z_relay(o, h).start()

    def along(o):
        z_wait(o, 0)
        side_copy(1, o, 0).start()
        z_wait(o, 1)
        side_copy(2, o, 1).start()
        side_copy(1, o, 1).start()
        side_copy(2, o, 0).start()

    def along_both():
        z_in(1, 0)
        side_copy(1, 1, 0).start()
        z_in(3, 0)
        side_copy(1, 3, 0).start()
        for o in (1, 3):
            z_in(o, 1)
            side_copy(2, o, 1).start()
            side_copy(1, o, 1).start()
            side_copy(2, o, 0).start()

    def dz_copy(o, h):
        here = inc.at[4 * z + 3, h]
        there = {"ep": 4 * at(o) + q}
        return remote(here, here, dz_send.at[0, o, h], link_recv.at[3, z, h], there)

    def dz_relay(o, h):
        j = at(o)
        here = inc.at[4 * j + 3, h]
        there = {"ep": 4 * at(4 - o) + q}
        return remote(here, here, dz_send.at[1, o, h], link_recv.at[3, j, h], there)

    def dz():
        for h in range(2):
            d_copy(h, 0).wait_recv()
            dz_copy(1, h).start()

            @pl.when(mid == 1)
            def _():
                dz_copy(3, h).start()

    def dzr():
        @pl.when(mid == 1)
        def _():
            for h in range(2):
                for o in (3, 1):
                    d_copy(h, o).wait_recv()
                    dz_relay(o, h).start()

    def near(o):
        for h in range(2):
            side_copy(1 + h, o, h).wait_recv()
            d_copy(h, o).start()

    def near_sides(o):
        side_copy(1, o, 0).wait_recv()
        side_copy(2, o, 1).wait_recv()

    spread = lax.broadcasted_iota(jnp.int32, (half, lanes), 0) + half * t == (
        lax.broadcasted_iota(jnp.int32, (half, lanes), 1)
    )

    def arrived_sides(o):
        side_copy(1, o, 1).wait_recv()
        side_copy(2, o, 0).wait_recv()

    def arrived(o):
        arrived_sides(o)
        if not (isinstance(o, int) and o == 0):
            for h in range(2):
                d_copy(h, o).wait_recv()

    def arr_end(o):
        arrived_sides(o)

        @pl.when(mid == 0)
        def _():
            for h in range(2):
                d_copy(h, o).wait_recv()

    def serve(o):
        slot = 4 * at(o)
        part = pl.ds(slot, 4)
        cols = []
        for r in range(4):
            cols.append(jnp.sum(jnp.where(spread, wrecv[slot + r], 0.0), axis=1, keepdims=True))
        scale = jnp.concatenate(cols, axis=0)
        low = inc[part, 0].reshape(4 * half, width)
        high = inc[part, 1].reshape(4 * half, width)
        hidden = []
        for gate_e, up_e in ((eg, eu), (eg_peer, eu_peer)):
            gate = dot(low, gate_e[0]) + dot(high, gate_e[1])
            up = dot(low, up_e[0]) + dot(high, up_e[1])
            hidden.append((jax.nn.silu(gate) * up).astype(BF16))
        for h, down in ((t, ed), (1 - t, ed_peer)):
            served = (dot(hidden[0], down[t]) + dot(hidden[1], down[1 - t])) * scale
            snd[part, h] = served.astype(BF16).reshape(4, half, width)

    def d_back(h, o):
        j = at(o)
        return remote(
            snd.at[4 * j + 3, h],
            got_d.at[j, h],
            back_send.at[3, j, h],
            back_recv.at[3, j, h],
            {"ep": x_near if h else y_near},
        )

    def side_back(r, o, h):
        j = at(o)
        near_chip = x_near if r == 1 else y_near
        if isinstance(o, int) and o == 0:
            return remote(
                snd.at[4 * j + r, h],
                (fin_x if r == 1 else fin_y).at[mine],
                back_send.at[r, j, h],
                fin_recv.at[r, t],
                {"ep": near_chip, "tp": h},
            )
        return remote(
            snd.at[4 * j + r, h],
            (got_x if r == 1 else got_y).at[j, h],
            back_send.at[r, j, h],
            back_recv.at[r, j, h],
            {"ep": near_chip},
        )

    def dz_back(o, h):
        j = at(o)
        there = {"ep": 4 * j + q}
        return remote(
            snd.at[4 * j + 3, h], got_dz.at[z, h], dz_send.at[3, o, h], dz_recv.at[z, h], there
        )

    def merge(slot, h, *parts):
        total = snd[slot, h].astype(F32)
        for part in parts:
            total = total + part.astype(F32)
        snd[slot, h] = total.astype(BF16)

    def send_all(o):
        for h in range(2):
            side_back(1, o, h).start()
            side_back(2, o, 1 - h).start()

    def send_first(o):
        d_back(0, o).start()
        d_back(1, o).start()
        side_back(1, o, 1).start()
        side_back(2, o, 0).start()

    def joined(o):
        j = at(o)
        for h in range(2):
            d_back(h, o).wait_recv()
            merge(4 * j + 1 + h, h, got_d[j, h])
            side_back(1 + h, o, h).start()

    def dz_wait(o, h):
        j = at(o)
        here = got_dz.at[j, h]
        remote(here, here, dz_send.at[3, o, h], dz_recv.at[j, h], partner).wait_recv()

    def send_own():
        @pl.when(mid == 1)
        def _():
            for h in range(2):
                dz_wait(3, h)
                dz_wait(2, h)
                merge(4 * z + 3, h, got_dz[at(3), h], got_dz[at(2), h])

        for h in range(2):
            dz_wait(1, h)
            merge(4 * z + 3, h, got_dz[at(1), h])
            d_back(h, 0).start()

    def bz_copy(o, h):
        j = at(o)
        return remote(
            zbuf.at[j, h],
            got_z.at[z, mine],
            back_send.at[0, j, h],
            back_recv.at[0, z, t],
            {"ep": 4 * j + q, "tp": h},
        )

    def bz_wait(o, core):
        j = at(o)
        here = got_z.at[j, pl.ds(core * half, half)]
        remote(here, here, back_send.at[0, j, 0], back_recv.at[0, j, core], partner).wait_recv()

    def home(o):
        j = at(o)
        for h in range(2):
            side_back(1, o, h).wait_recv()
            side_back(2, o, h).wait_recv()
            total = snd[4 * j, h].astype(F32) + got_x[j, h].astype(F32) + got_y[j, h].astype(F32)
            zbuf[j, h] = total.astype(BF16)
            bz_copy(o, h).start()

    own_copy = remote(snd.at[4 * z, 1 - t], fin_o, fin_send.at[0], fin_recv.at[0, 0], partner)

    for o in (1, 3):
        for h in range(2):
            z_copy(o, h).start()
    sides(0)
    pushes[1].start()
    pushes[2].start()

    for load in loads[14:18]:
        load.wait()
    res_copy(other, 1).wait_recv()
    norm_part(other)
    dense_gate = dot(nrm_ref[0], dg[t]) + dot(nrm_ref[1], dg[1 - t])
    dense_up = dot(nrm_ref[0], du[t]) + dot(nrm_ref[1], du[1 - t])
    dhid[0] = (jax.nn.silu(dense_gate) * dense_up).astype(BF16)
    dense_copy = remote(dhid.at[0], dhid.at[1], m_send.at[2], m_recv.at[2], partner)
    dense_copy.start()
    near(0)

    @pl.when(mid == 1)
    def _():
        along_both()

    @pl.when(mid == 0)
    def _():
        along(1)

    for r, o in places:
        slot = 4 * ((z + o) % depth) + r
        remote(wsend.at[0], wrecv.at[slot], w_send.at[0], w_recv.at[slot], partner).wait_recv()
    row = jnp.sum(jnp.where(ids == e, weights, 0.0), axis=0, keepdims=True)
    wrecv[4 * z] = jnp.concatenate([row, jnp.zeros((1, lanes - rows), F32)], axis=1)
    dense = dot(dhid[0], dd[t])
    dense_copy.wait_recv()
    dense = (dense + dot(dhid[1], dd[1 - t])).astype(BF16)
    base_ref[...] = resid + scale_ref[...] * dense.astype(F32)
    for load in loads[18:]:
        load.wait()
    for push in pushes:
        push.wait_recv()

    @pl.when(mid == 0)
    def _():
        along(3)

    dz()
    along(2)
    arrived(0)
    serve(0)
    own_copy.start()
    dzr()

    @pl.when(mid == 0)
    def _():
        near(3)


    @pl.when(mid == 1)
    def _():
        near_sides(2)

    near_sides(1)
    arr_end(1)
    serve(1)
    dz_back(1, 0).start()
    dz_back(1, 1).start()
    side_back(1, 1, 0).start()
    side_back(2, 1, 1).start()

    @pl.when(mid == 1)
    def _():
        near_sides(3)
        arrived_sides(3)


    @pl.when(mid == 0)
    def _():
        arrived(3)

    serve(3)

    @pl.when(mid == 1)
    def _():
        dz_back(3, 0).start()
        dz_back(3, 1).start()


    @pl.when(mid == 0)
    def _():
        send_first(3)

    side_back(1, 1, 1).start()
    side_back(2, 1, 0).start()

    @pl.when(mid == 0)
    def _():
        near_sides(2)

    arrived(2)
    serve(2)

    @pl.when(mid == 0)
    def _():
        dz_back(2, 0).start()
        dz_back(2, 1).start()


    @pl.when(mid == 1)
    def _():
        send_first(2)
        side_back(1, 3, 0).start()
        side_back(2, 3, 1).start()


    @pl.when(mid == 1)
    def _():
        home(1)

    joined(o_c)

    @pl.when(mid == 0)
    def _():
        send_all(2)


    @pl.when(mid == 1)
    def _():
        side_back(1, 3, 1).start()
        side_back(2, 3, 0).start()

    side_back(1, 0, 1).start()
    side_back(2, 0, 0).start()

    @pl.when(mid == 0)
    def _():
        home(1)

    send_own()
    home(o_c)
    home(o_b)
    joined(0)
    base_ref[mine, :] += snd[4 * z, t].astype(F32)
    own_copy.wait_recv()
    base_ref[other, :] += fin_o[...].astype(F32)
    total = base_ref[...]
    for o in (1, 3, 2):
        for core in range(2):
            bz_wait(o, core)
        total = total + got_z[at(o)].astype(F32)
    for r, fin in ((1, fin_x), (2, fin_y)):
        for core in range(2):
            here = fin.at[pl.ds(core * half, half)]
            remote(here, here, fin_send.at[1], fin_recv.at[r, core], partner).wait_recv()
        total = total + fin[...].astype(F32)
    result_ref[...] = total.astype(BF16)
    stores.append(pltpu.make_async_copy(result_ref, result_hbm, store_sem.at[2]))
    stores[-1].start()
    res_copy(other, 0).wait_send()
    res_copy(mine, 1).wait_send()
    for copy in (first, dense_copy, own_copy, second, *pushes):
        copy.wait_send()
    for r, o in places:
        weighing(r, o).wait_send()
    for o in range(depth):
        for h in range(2):
            if o:
                bz_copy(o, h).wait_send()
            if o in (1, 3):
                z_copy(o, h).wait_send()
            for r in (1, 2):
                side_copy(r, o, h).wait_send()
                side_back(r, o, h).wait_send()
        if o == 0:
            for h in range(2):
                d_copy(h, o).wait_send()
                d_back(h, o).wait_send()

    @pl.when(mid == 1)
    def _():
        for h in range(2):
            z_relay(1, h).wait_send()
            z_relay(3, h).wait_send()
            dz_relay(1, h).wait_send()
            dz_relay(3, h).wait_send()
            dz_copy(3, h).wait_send()
            dz_back(3, h).wait_send()

    @pl.when(mid == 0)
    def _():
        for h in range(2):
            dz_back(2, h).wait_send()
            d_copy(h, 3).wait_send()

    for h in range(2):
        d_back(h, o_c).wait_send()
        dz_copy(1, h).wait_send()
        dz_back(1, h).wait_send()

    for store in stores:
        store.wait()


def expert_kernel(
    full,
    peers,
    group,
    n2_ref,
    out_ref,
    resid_ref,
    ids_ref,
    weights_ref,
    scale_ref,
    eg_hbm,
    eu_hbm,
    ed_hbm,
    dg_hbm,
    du_hbm,
    dd_hbm,
    *refs,
):
    if full:
        result_ref, *refs = refs
    else:
        dense_ref, back_ref, *refs = refs
    (
        eg,
        eu,
        ed,
        dg,
        du,
        dd,
        inc,
        hid,
        src,
        ret,
        dhid,
        load_sem,
        own_sem,
        x_send,
        x_recv,
        f_send,
        f_recv,
        h_send,
        h_recv,
        r_send,
        r_recv,
        d_sem,
    ) = refs
    e = lax.axis_index("ep")
    t = lax.axis_index("tp")
    partner = {"tp": 1 - t}
    groups = peers // group
    cap = inc.shape[2]
    width = inc.shape[3]
    loads = [
        pltpu.make_async_copy(a, b, load_sem.at[i])
        for i, (a, b) in enumerate(
            ((dg_hbm, dg), (du_hbm, du), (dd_hbm, dd), (eg_hbm, eg), (eu_hbm, eu), (ed_hbm, ed))
        )
    ]
    for load in loads:
        load.start()

    def outgoing(offset):
        return n2_ref.at[0] if full else out_ref.at[lax.rem(e + offset, peers)]

    keep = pltpu.make_async_copy(outgoing(0), inc.at[0, 0], own_sem)
    keep.start()
    barrier = pltpu.get_barrier_semaphore()
    pl.semaphore_signal(barrier, inc=1, device_id=partner, device_id_type=pl.DeviceIdType.MESH)

    @pl.loop(1, peers)
    def _(offset):
        pl.semaphore_signal(
            barrier,
            inc=1,
            device_id={"ep": lax.rem(e + offset, peers)},
            device_id_type=pl.DeviceIdType.MESH,
        )

    pl.semaphore_wait(barrier, peers)

    def sending(offset):
        return remote(
            outgoing(offset),
            inc.at[0, offset],
            x_send.at[offset],
            x_recv.at[offset],
            {"ep": lax.rem(e + offset, peers)},
        )

    @pl.loop(1, peers)
    def _(offset):
        sending(offset).start()

    for load in loads[:3]:
        load.wait()
    rows0, rows1 = n2_ref[0], n2_ref[1]
    dense_gate = dot(rows0, dg[t]) + dot(rows1, dg[1 - t])
    dense_up = dot(rows0, du[t]) + dot(rows1, du[1 - t])
    dhid[0] = (jax.nn.silu(dense_gate) * dense_up).astype(BF16)
    dense_copy = remote(dhid.at[0], dhid.at[1], d_sem.at[0], d_sem.at[1], partner)
    dense_copy.start()
    dense = dot(dhid[0], dd[t])
    dense_copy.wait()
    dense = (dense + dot(dhid[1], dd[1 - t])).astype(BF16)
    keep.wait()
    for load in loads[3:]:
        load.wait()

    def forwarding(g):
        part = pl.ds(g * group, group)
        return remote(inc.at[0, part], inc.at[1, part], f_send.at[g], f_recv.at[g], partner)

    def hiding(g):
        part = pl.ds(g * group, group)
        return remote(hid.at[0, part], hid.at[1, part], h_send.at[g], h_recv.at[g], partner)

    def returning(offset):
        return remote(
            src.at[offset],
            ret.at[offset],
            r_send.at[offset],
            r_recv.at[offset],
            {"ep": lax.rem(e + peers - offset, peers)},
        )

    def arrive(g):
        @pl.loop(max(1, g * group), (g + 1) * group)
        def _(offset):
            sending(offset).wait_recv()

        forwarding(g).start()

    def upward(g):
        forwarding(g).wait_recv()
        part = pl.ds(g * group, group)
        own = inc[0, part].reshape(group * cap, width)
        peer = inc[1, part].reshape(group * cap, width)
        gate = dot(own, eg[t]) + dot(peer, eg[1 - t])
        up = dot(own, eu[t]) + dot(peer, eu[1 - t])
        hidden = (jax.nn.silu(gate) * up).astype(BF16)
        hid[0, part] = hidden.reshape(group, cap, -1)
        hiding(g).start()

    def downward(g):
        hiding(g).wait_recv()
        part = pl.ds(g * group, group)
        own = hid[0, part].reshape(group * cap, -1)
        peer = hid[1, part].reshape(group * cap, -1)
        served = dot(own, ed[t]) + dot(peer, ed[1 - t])
        src[part] = served.astype(BF16).reshape(group, cap, width)

        @pl.loop(max(1, g * group), (g + 1) * group)
        def _(offset):
            returning(offset).start()

    for step in range(groups + 2):
        if step < groups:
            arrive(step)
        if 1 <= step <= groups:
            upward(step - 1)
        if step >= 2:
            downward(step - 2)

    if full:
        total = resid_ref[...].astype(F32) + scale_ref[...] * dense.astype(F32)
        ids = ids_ref[...]
        weights = weights_ref[...]

        def weight(offset):
            chosen = ids == lax.rem(e + offset, peers)
            return jnp.sum(jnp.where(chosen, weights, 0.0), axis=1, keepdims=True)

        routed = weight(0) * src[0].astype(F32)
        for offset in range(1, peers):
            returning(offset).wait_recv()
            routed = routed + weight(offset) * ret[offset].astype(F32)
        result_ref[...] = (total + routed).astype(BF16)
    else:
        dense_ref[...] = dense
        back_ref[0] = src[0]

        @pl.loop(1, peers)
        def _(offset):
            returning(offset).wait_recv()
            back_ref[offset] = ret[offset]

    @pl.loop(1, peers)
    def _(offset):
        sending(offset).wait_send()
        returning(offset).wait_send()

    @pl.loop(0, groups)
    def _(g):
        forwarding(g).wait_send()
        hiding(g).wait_send()


def emit_kernel(a_in, b_in, c_in, a_out, b_out, c_out, a, b, c, sem):
    sets = tuple(enumerate(((a_in, a, a_out), (b_in, b, b_out), (c_in, c, c_out))))
    reads = [pltpu.make_async_copy(src, mid, sem.at[0, i]) for i, (src, mid, _) in sets]
    writes = [pltpu.make_async_copy(mid, dst, sem.at[1, i]) for i, (_, mid, dst) in sets]
    for read in reads:
        read.start()
    for read, write in zip(reads, writes):
        read.wait()
        write.start()
    for write in writes:
        write.wait()


def halves(weight):
    return weight.reshape(2, weight.shape[0] // 2, weight.shape[1])


def per_device(
    stream,
    conv_state,
    recur_state,
    mix_gain,
    branch_weight,
    gate_weight,
    conv_taps,
    recur_map,
    input_map,
    decay_logit,
    out_weight,
    moe_gain,
    route_ids,
    route_weights,
    expert_gate,
    expert_up,
    expert_down,
    dense_gate,
    dense_up,
    dense_down,
    dense_scale,
):
    rows, width = stream.shape
    dma = pltpu.SemaphoreType.DMA
    top = route_ids.shape[1]
    peers = lax.axis_size("ep")
    cap = max(2, min(rows, 3 * rows * top // peers))
    if cap == rows and peers // 4 == 4:
        operands = (
            stream,
            conv_state.transpose(1, 0, 2),
            recur_state,
            mix_gain.reshape(2, 1, width),
            halves(branch_weight),
            halves(gate_weight),
            conv_taps,
            recur_map,
            input_map,
            decay_logit.reshape(1, width),
            halves(out_weight),
            moe_gain.reshape(2, 1, width),
            route_ids.T,
            route_weights.T,
            dense_scale.reshape(1, width),
            halves(expert_gate[0]),
            halves(expert_up[0]),
            halves(expert_down[0]),
            halves(dense_gate),
            halves(dense_up),
            halves(dense_down),
        )
        depth = peers // 4
        half = rows // 2
        lanes = -(-rows // 128) * 128
        outs = (
            jax.ShapeDtypeStruct((rows, width), BF16),
            jax.ShapeDtypeStruct((rows, width), F32),
            jax.ShapeDtypeStruct((3, rows, width), BF16),
        )
        column = pltpu.VMEM((depth, 2, half, width), BF16)
        whole = pltpu.VMEM((rows, width), BF16)
        result, new_state, new_conv = pl.pallas_call(
            functools.partial(layer_kernel, peers),
            out_shape=outs,
            in_specs=[ANY] * len(operands),
            out_specs=[ANY] * 3,
            scratch_shapes=[pltpu.VMEM(a.shape, a.dtype) for a in operands + outs + operands[15:18]]
            + [whole]
            + [pltpu.VMEM((2, rows, width), BF16)] * 3
            + [pltpu.VMEM((2, rows, dense_gate.shape[1]), BF16)]
            + [pltpu.VMEM((peers, 2, half, width), BF16)] * 2
            + [column] * 5
            + [pltpu.VMEM((depth, rows, width), BF16)]
            + [whole] * 2
            + [pltpu.VMEM((half, width), BF16), pltpu.VMEM((rows, width), F32)]
            + [pltpu.VMEM((peers, 1, lanes), F32)] * 2
            + [dma((len(operands),)), dma((3,))]
            + [dma((3,))] * 2
            + [dma((1,))] * 2
            + [dma((3,))] * 2
            + [dma((peers,))] * 2
            + [dma((4, depth, 2))] * 4
            + [dma((2,)), dma((3, 2)), dma((4, depth, 2)), dma((depth, 2))]
            + [dma((2,))] * 2,
            compiler_params=pltpu.CompilerParams(
                collective_id=2, has_side_effects=True, vmem_limit_bytes=63 * 1024 * 1024
            ),
            name="layer",
        )(*operands)
        result, new_state, new_conv = pl.pallas_call(
            emit_kernel,
            out_shape=tuple(jax.ShapeDtypeStruct(a.shape, a.dtype) for a in (result, new_state, new_conv)),
            in_specs=[ANY] * 3,
            out_specs=[ANY] * 3,
            scratch_shapes=[pltpu.VMEM(a.shape, a.dtype) for a in (result, new_state, new_conv)]
            + [dma((2, 3))],
            compiler_params=pltpu.CompilerParams(vmem_limit_bytes=63 * 1024 * 1024),
            name="emit",
        )(result, new_state, new_conv)
        return result, new_state, new_conv.transpose(1, 0, 2)
    conv_part = sum(conv_state[:, i].astype(F32) * conv_taps[i] for i in range(3))
    branch_in, new_state, resid, n2 = pl.pallas_call(
        mixer_kernel,
        out_shape=(
            jax.ShapeDtypeStruct((rows, width), BF16),
            jax.ShapeDtypeStruct((rows, width), F32),
            jax.ShapeDtypeStruct((rows, width), BF16),
            jax.ShapeDtypeStruct((2, rows, width), BF16),
        ),
        in_specs=[VMEM] * 4 + [ANY] * 2 + [VMEM] * 4 + [ANY, VMEM],
        out_specs=[VMEM] * 4,
        scratch_shapes=[pltpu.VMEM((2, width, width), BF16)] * 3
        + [pltpu.VMEM((rows, width), BF16)]
        + [pltpu.VMEM((2, rows, width), BF16)] * 3
        + [dma((3,))] * 3,
        compiler_params=pltpu.CompilerParams(
            collective_id=0, has_side_effects=True, vmem_limit_bytes=48 * 1024 * 1024
        ),
        name="mixer",
    )(
        stream,
        conv_part,
        recur_state,
        mix_gain.reshape(2, 1, width),
        halves(branch_weight),
        halves(gate_weight),
        conv_taps,
        recur_map,
        input_map,
        decay_logit.reshape(1, width),
        halves(out_weight),
        moe_gain.reshape(2, 1, width),
    )
    new_conv = jnp.concatenate([conv_state[:, 1:], branch_in[:, None]], axis=1)

    full = cap == rows
    if full:
        outgoing = jnp.zeros((8, 128), BF16)
    else:
        cap = -(-cap // 16) * 16
        flat_ids = route_ids.reshape(-1)
        one_hot = (flat_ids[:, None] == jnp.arange(peers, dtype=jnp.int32)[None, :]).astype(jnp.int32)
        rank = jnp.sum(one_hot * (jnp.cumsum(one_hot, axis=0) - 1), axis=1)
        slots = (flat_ids * cap + rank).reshape(rows, top)
        table = jnp.sum(
            (slots[:, :, None] == jnp.arange(peers * cap, dtype=jnp.int32)).astype(BF16), axis=1
        )
        outgoing = lax.dot_general(
            table, n2[0], (((0,), (0,)), ((), ())), preferred_element_type=F32
        )
        outgoing = outgoing.astype(BF16).reshape(peers, cap, width)
    group = max(1, min(peers, 256 // cap))
    while peers % group:
        group -= 1
    groups = peers // group
    hidden = expert_gate.shape[2]
    out_shape = [jax.ShapeDtypeStruct((rows, width), BF16)]
    if not full:
        out_shape.append(jax.ShapeDtypeStruct((peers, cap, width), BF16))
    outs = pl.pallas_call(
        functools.partial(expert_kernel, full, peers, group),
        out_shape=out_shape,
        in_specs=[VMEM] * 6 + [ANY] * 6,
        out_specs=[VMEM] * len(out_shape),
        scratch_shapes=[
            pltpu.VMEM((2, width, hidden), BF16),
            pltpu.VMEM((2, width, hidden), BF16),
            pltpu.VMEM((2, hidden, width), BF16),
            pltpu.VMEM((2, width, dense_gate.shape[1]), BF16),
            pltpu.VMEM((2, width, dense_gate.shape[1]), BF16),
            pltpu.VMEM((2, dense_gate.shape[1], width), BF16),
            pltpu.VMEM((2, peers, cap, width), BF16),
            pltpu.VMEM((2, peers, cap, hidden), BF16),
            pltpu.VMEM((peers, cap, width), BF16),
            pltpu.VMEM((peers, cap, width), BF16),
            pltpu.VMEM((2, rows, dense_gate.shape[1]), BF16),
            dma((6,)),
            dma,
            dma((peers,)),
            dma((peers,)),
            dma((groups,)),
            dma((groups,)),
            dma((groups,)),
            dma((groups,)),
            dma((peers,)),
            dma((peers,)),
            dma((2,)),
        ],
        compiler_params=pltpu.CompilerParams(
            collective_id=1, has_side_effects=True, vmem_limit_bytes=56 * 1024 * 1024
        ),
        name="experts",
    )(
        n2,
        outgoing,
        resid,
        route_ids,
        route_weights,
        dense_scale.reshape(1, width),
        halves(expert_gate[0]),
        halves(expert_up[0]),
        halves(expert_down[0]),
        halves(dense_gate),
        halves(dense_up),
        halves(dense_down),
    )
    if full:
        return outs[0], new_state, new_conv
    dense_out, back = outs
    shifted = lax.rem(flat_ids - lax.axis_index("ep") + peers, peers)
    picked = back.reshape(peers * cap, width)[(shifted * cap + rank).reshape(rows, top)]
    routed = jnp.sum(picked.astype(F32) * route_weights[:, :, None], axis=1)
    result = (resid.astype(F32) + routed + dense_scale * dense_out.astype(F32)).astype(BF16)
    return result, new_state, new_conv


def solution(mesh):
    in_specs = (
        P("ep", "tp"),
        P("ep", None, "tp"),
        P("ep", "tp"),
        P(),
        P(None, "tp"),
        P(None, "tp"),
        P(None, "tp"),
        P("tp", None, None),
        P("tp", None, None),
        P("tp"),
        P(None, "tp"),
        P(),
        P("ep", None),
        P("ep", None),
        P("ep", None, "tp"),
        P("ep", None, "tp"),
        P("ep", None, "tp"),
        P(None, "tp"),
        P(None, "tp"),
        P(None, "tp"),
        P("tp"),
    )
    out_specs = (P("ep", "tp"), P("ep", "tp"), P("ep", None, "tp"))
    return jax.shard_map(
        per_device, mesh=mesh, in_specs=in_specs, out_specs=out_specs, check_vma=False
    )
```
